128 devices in a mesh: sp: 32 (over z, y, core), tp: 4 (over x).
Axes of the slice: x: 4, y: 4, z: 4, core: 2. Of those that a mesh axis runs over, the one named last changes fastest.
Arguments:
- residual: bfloat16 [32768, 2048], P('sp'), may hold values from -8 to 8
- query_wide: bfloat16 [32768, 1024], P('sp', 'tp'), may hold values from -6 to 6
- key_wide: bfloat16 [32768, 1024], P('sp', 'tp'), may hold values from -6 to 6
- value_wide: bfloat16 [32768, 2048], P('sp', 'tp'), may hold values from -6 to 6
- decay_wide: bfloat16 [32768, 1024], P('sp', 'tp'), may hold values from -12 to 12
- gate_wide: bfloat16 [32768, 2048], P('sp', 'tp'), may hold values from -6 to 6
- query_narrow: bfloat16 [32768, 512], P('sp', 'tp'), may hold values from -6 to 6
- key_narrow: bfloat16 [32768, 512], P('sp', 'tp'), may hold values from -6 to 6
- value_narrow: bfloat16 [32768, 2048], P('sp', 'tp'), may hold values from -6 to 6
- decay_narrow: bfloat16 [32768, 512], P('sp', 'tp'), may hold values from -12 to 12
- gate_narrow: bfloat16 [32768, 2048], P('sp', 'tp'), may hold values from -6 to 6
- head_gain: float32 [512], replicated, may hold values from 0.1 to 1.9
- out_wide: bfloat16 [2048, 2048], P('tp'), may hold values from -0.125 to 0.125
- out_narrow: bfloat16 [2048, 2048], P('tp'), may hold values from -0.125 to 0.125
- mlp_gain: float32 [2048], replicated, may hold values from 0.1 to 1.9
- up_weight: bfloat16 [2048, 4096], P('sp', 'tp'), may hold values from -0.125 to 0.125
- down_weight: bfloat16 [4096, 2048], P('tp', 'sp'), may hold values from -0.09375 to 0.09375
Outputs:
- layer_out: bfloat16 [32768, 2048], P('sp', 'tp')
The draws below stay inside these ranges and needn't reach their ends.
All inputs are finite; a program needn't handle non-finite values.
Results may differ from the reference program's by a relative error of at most 0.017.
Values may be sent and summed in bfloat16 or wider, within the bound.
No kernel may reach another device: no remote copies, remote signals or barrier semaphores. Data moves between devices by JAX's collectives and lax.ppermute only.
A program may use at most 128 MiB of HBM per device.

```python
import math
import jax
import jax.numpy as jnp
from jax import lax

D = 2048
FF = 4096
HEADS = 4
HEAD_KA = 256
HEAD_KB = 128
HEAD_V = 512
BLOCK = 64
TOK_DEV = 1024
SEQUENCE_TOKENS = 32768
N_TP = 4


def draw_residual(key, part):
    column = jnp.arange(D, dtype=jnp.float32) / D
    baseline = jax.random.normal(jax.random.fold_in(key, 3), (SEQUENCE_TOKENS, D), jnp.float32)
    scale = 0.5 * jnp.power(4.0, column)
    return jnp.clip(baseline * scale[None, :], -8.0, 8.0).astype(jnp.bfloat16)


def decay_draw(key, head_width, salt):
    random_subkeys = jax.random.split(jax.random.fold_in(key, salt), 6)
    channel_count = HEADS * head_width
    ranking = jax.random.permutation(random_subkeys[0], HEADS)
    slow_heads = ranking < HEADS // 2
    jitter = jnp.clip(jax.random.normal(random_subkeys[1], (SEQUENCE_TOKENS, channel_count), jnp.float32), -3.0, 3.0)
    offsets = jax.random.uniform(random_subkeys[2], (SEQUENCE_TOKENS // TOK_DEV,), jnp.float32, -0.7, 0.7)
    slow_cols = jnp.repeat(slow_heads, head_width, total_repeat_length=channel_count)
    baseline = jnp.where(slow_cols, math.log(SEQUENCE_TOKENS / 4.0), 1.0)
    spread = jax.random.uniform(random_subkeys[3], (channel_count,), jnp.float32, -0.5, 0.5)
    grouped_rows = jax.random.randint(random_subkeys[4], (3,), 0, SEQUENCE_TOKENS)
    group_match = jnp.any(jnp.arange(SEQUENCE_TOKENS)[:, None] == grouped_rows[None, :], axis=1)
    group_depth = jax.random.uniform(random_subkeys[5], (SEQUENCE_TOKENS, 1), jnp.float32, 3.5, 8.0)
    row_offsets = jnp.repeat(offsets, TOK_DEV, total_repeat_length=SEQUENCE_TOKENS)
    before_activation = baseline[None, :] + spread[None, :] + row_offsets[:, None] + jitter
    before_activation = jnp.where(group_match[:, None], -group_depth, before_activation)
    return jnp.clip(before_activation, -12.0, 12.0).astype(jnp.bfloat16)


def draw_decay_wide(key, part):
    return decay_draw(key, HEAD_KA, 11)


def draw_decay_narrow(key, part):
    return decay_draw(key, HEAD_KB, 13)


def levels(rng, extent, pieces, least, largest):
    def one(dim, blocks):
        draws = jax.random.uniform(jax.random.fold_in(jax.random.fold_in(rng, 6), dim), (blocks,), jnp.float32, least / len(pieces), largest / len(pieces))
        return jnp.repeat(jnp.exp(draws), extent[dim] // blocks).reshape((-1,) + (1,) * (len(extent) - dim - 1))

    factor_of = one(*pieces[0])
    for cut in pieces[1:]:
        factor_of = factor_of * one(*cut)
    return factor_of


def centred(own_key, extent, scale, bound, pieces=(), kind=jnp.bfloat16):
    gain = levels(own_key, extent, pieces, -0.22, 0.18) if pieces else 1.0
    drawn = jax.random.normal(own_key, extent, jnp.float32) * scale * gain
    return jnp.minimum(jnp.maximum(drawn, -bound), bound).astype(kind)


def setup_inputs(seed: int = 0) -> dict:
    streams_of = jax.random.split(jax.random.key(seed), 18)
    residual = draw_residual(jax.random.fold_in(streams_of[17], 71), 0)
    query_wide = centred(streams_of[1], (SEQUENCE_TOKENS, HEADS * HEAD_KA), 1.0, 6.0, ((0, 32), (1, 4)))
    key_wide = centred(streams_of[2], (SEQUENCE_TOKENS, HEADS * HEAD_KA), 1.0, 6.0, ((0, 32), (1, 4)))
    value_wide = centred(streams_of[3], (SEQUENCE_TOKENS, HEADS * HEAD_V), 1.0, 6.0, ((0, 32), (1, 4)))
    decay_wide = draw_decay_wide(jax.random.fold_in(streams_of[17], 71), 0)
    gate_wide = centred(streams_of[5], (SEQUENCE_TOKENS, HEADS * HEAD_V), 1.0, 6.0, ((0, 32), (1, 4)))
    query_narrow = centred(streams_of[6], (SEQUENCE_TOKENS, HEADS * HEAD_KB), 1.0, 6.0, ((0, 32), (1, 4)))
    key_narrow = centred(streams_of[7], (SEQUENCE_TOKENS, HEADS * HEAD_KB), 1.0, 6.0, ((0, 32), (1, 4)))
    value_narrow = centred(streams_of[8], (SEQUENCE_TOKENS, HEADS * HEAD_V), 1.0, 6.0, ((0, 32), (1, 4)))
    decay_narrow = draw_decay_narrow(jax.random.fold_in(streams_of[17], 71), 0)
    gate_narrow = centred(streams_of[10], (SEQUENCE_TOKENS, HEADS * HEAD_V), 1.0, 6.0, ((0, 32), (1, 4)))
    head_gain = jnp.clip(1.0 + 0.18 * jax.random.normal(streams_of[11], (HEAD_V,), jnp.float32), 0.1, 1.9)
    out_wide = centred(streams_of[12], (HEADS * HEAD_V, D), (HEADS * HEAD_V) ** -0.5, 0.125, ((0, 4),))
    out_narrow = centred(streams_of[13], (HEADS * HEAD_V, D), (HEADS * HEAD_V) ** -0.5, 0.125, ((0, 4),))
    mlp_gain = jnp.clip(1.0 + 0.18 * jax.random.normal(streams_of[14], (D,), jnp.float32), 0.1, 1.9)
    up_weight = centred(streams_of[15], (D, FF), D ** -0.5, 0.125, ((0, 32), (1, 4)))
    down_weight = centred(streams_of[16], (FF, D), FF ** -0.5, 0.09375, ((0, 4), (1, 32)))
    return dict(residual=residual, query_wide=query_wide, key_wide=key_wide, value_wide=value_wide, decay_wide=decay_wide, gate_wide=gate_wide, query_narrow=query_narrow, key_narrow=key_narrow, value_narrow=value_narrow, decay_narrow=decay_narrow, gate_narrow=gate_narrow, head_gain=head_gain, out_wide=out_wide, out_narrow=out_narrow, mlp_gain=mlp_gain, up_weight=up_weight, down_weight=down_weight)


EPS = 1e-05
DECAY_NORMALIZER = 16.0
HIGHEST = lax.Precision.HIGHEST

def block_pass(queries, keys_in, values_in, log_decay, block_len):
    num_blocks = queries.shape[0] // block_len

    def to_blocks(stacked):
        return stacked.reshape((num_blocks, block_len) + stacked.shape[1:])
    causal = jnp.tril(jnp.ones((block_len, block_len), dtype=bool))
    initial = (jnp.zeros((queries.shape[1], queries.shape[2], values_in.shape[2]), jnp.float32), jnp.zeros((queries.shape[1], queries.shape[2]), jnp.float32))

    def advance(running, inputs):
        memory, offset = running
        block_q, block_k, block_v, block_g = inputs
        within = jnp.cumsum(block_g, axis=0)
        final_log = within[-1]
        scaled_q = block_q * jnp.exp(within)
        scaled_k = block_k * jnp.exp(-within)
        outside = jnp.einsum('ihd,hde->ihe', scaled_q, memory, precision=HIGHEST)
        scores = jnp.einsum('ihd,jhd->hij', scaled_q, scaled_k, precision=HIGHEST)
        scores = jnp.where(causal[None], scores, 0.0)
        inside = jnp.einsum('hij,jhe->ihe', scores, block_v, precision=HIGHEST)
        decayed_keys = scaled_k * jnp.exp(final_log)[None]
        memory = jnp.exp(final_log)[..., None] * memory + jnp.einsum('jhd,jhe->hde', decayed_keys, block_v, precision=HIGHEST)
        carried_q = scaled_q * jnp.exp(offset)[None]
        return ((memory, offset + final_log), (outside + inside, carried_q))
    (memory, totals), (outputs, carried_q) = lax.scan(advance, initial, (to_blocks(queries), to_blocks(keys_in), to_blocks(values_in), to_blocks(log_decay)))
    return (outputs.reshape(values_in.shape), carried_q.reshape(queries.shape), totals, memory)

def prepare(query, key_proj, value, decay, heads_here):
    row_count = query.shape[0]
    key_width = query.shape[1] // heads_here
    queries = query.astype(jnp.float32).reshape(row_count, heads_here, key_width) * key_width ** (-0.5)
    keys_in = key_proj.astype(jnp.float32).reshape(row_count, heads_here, key_width)
    values_in = value.astype(jnp.float32).reshape(row_count, heads_here, value.shape[1] // heads_here)
    log_decay = jax.nn.log_sigmoid(decay.astype(jnp.float32)).reshape(row_count, heads_here, key_width) / DECAY_NORMALIZER
    return (queries, keys_in, values_in, log_decay)

def finish(outputs, gate, head_gain):
    scale = lax.rsqrt(lax.optimization_barrier(jnp.mean(jnp.square(outputs), axis=-1, keepdims=True)) + EPS)
    gated = outputs * scale * head_gain * jax.nn.silu(gate.astype(jnp.float32).reshape(outputs.shape))
    return gated.reshape(outputs.shape[0], -1).astype(jnp.bfloat16)

def group_output(query, key_proj, value, decay, gate, head_gain):
    queries, keys_in, values_in, log_decay = prepare(query, key_proj, value, decay, HEADS)
    outputs = block_pass(queries, keys_in, values_in, log_decay, BLOCK)[0]
    return finish(outputs, gate, head_gain)

def blockwise_sum(left_sides, right_sides):
    total = jnp.zeros((left_sides[0].shape[0], right_sides[0].shape[1]), jnp.float32)
    for tp_block in range(N_TP):
        block_sum = jnp.zeros_like(total)
        for left_side, right_side in zip(left_sides, right_sides):
            block_width = left_side.shape[1] // N_TP
            first_col = tp_block * block_width
            block_sum = block_sum + jnp.dot(left_side[:, first_col:first_col + block_width], right_side[first_col:first_col + block_width], preferred_element_type=jnp.float32)
        total = total + lax.optimization_barrier(block_sum.astype(jnp.bfloat16)).astype(jnp.float32)
    return total

def reference(residual, query_wide, key_wide, value_wide, decay_wide, gate_wide, query_narrow, key_narrow, value_narrow, decay_narrow, gate_narrow, head_gain, out_wide, out_narrow, mlp_gain, up_weight, down_weight):
    gated_wide = group_output(query_wide, key_wide, value_wide, decay_wide, gate_wide, head_gain)
    gated_narrow = group_output(query_narrow, key_narrow, value_narrow, decay_narrow, gate_narrow, head_gain)
    mixed = blockwise_sum((gated_wide, gated_narrow), (out_wide, out_narrow))
    stream = (residual.astype(jnp.float32) + mixed).astype(jnp.bfloat16)
    stream_f = stream.astype(jnp.float32)
    normed = (stream_f * lax.rsqrt(lax.optimization_barrier(jnp.mean(jnp.square(stream_f), axis=1, keepdims=True)) + EPS) * mlp_gain).astype(jnp.bfloat16)
    hidden = jnp.square(jax.nn.relu(jnp.dot(normed, up_weight, preferred_element_type=jnp.float32))).astype(jnp.bfloat16)
    mlp_sum = blockwise_sum((hidden,), (down_weight,))
    return (stream_f + mlp_sum).astype(jnp.bfloat16)
```

```python
import functools

import jax
import jax.numpy as jnp
from jax import lax
from jax.experimental import pallas as pl
from jax.experimental.pallas import tpu as pltpu
from jax.sharding import PartitionSpec as P

EPS = 1e-05
DECAY_NORMALIZER = 16.0
CHUNK = 128
F32 = jnp.float32
BF16 = jnp.bfloat16
NT = (((1,), (1,)), ((), ()))
TN = (((0,), (0,)), ((), ()))
E_ROWS = 8


def dot(a, b, dims=(((1,), (0,)), ((), ()))):
    return lax.dot_general(a, b, dims, preferred_element_type=F32)


def log_decay_of(pre):
    x = pre.astype(F32)
    return (jnp.minimum(x, 0.0) - jnp.log1p(jnp.exp(-jnp.abs(x)))) / DECAY_NORMALIZER


def tri_sum(tri, g):
    high = g.astype(BF16)
    low = (g - high.astype(F32)).astype(BF16)
    return dot(tri, high) + dot(tri, low)


def tri_mask(kind):
    row = lax.broadcasted_iota(jnp.int32, (CHUNK, CHUNK), 0)
    col = lax.broadcasted_iota(jnp.int32, (CHUNK, CHUNK), 1)
    return (col <= row) if kind == "lower" else (col > row)


def params(**kw):
    return pltpu.CompilerParams(vmem_limit_bytes=56 * 1024 * 1024, **kw)


def state_kernel(kw, dw, vw, kn, dn, vn, packed, decayed_w, decayed_n):
    later = tri_mask("upper").astype(BF16)
    rows = kw.shape[0]
    keys_w = kw.shape[1]
    for key, pre, decayed, value, at in (
        (kw, dw, decayed_w, vw, 0),
        (kn, dn, decayed_n, vn, keys_w),
    ):
        width = key.shape[1]
        offset = jnp.zeros((1, width), F32)
        for block in reversed(range(rows // CHUNK)):
            span = pl.ds(block * CHUNK, CHUNK)
            g = log_decay_of(pre[span, :])
            after = tri_sum(later, g)
            decayed[span, :] = (key[span, :].astype(F32) * jnp.exp(after + offset)).astype(BF16)
            offset = offset + after[0:1, :] + g[0:1, :]
        state = dot(value[...], decayed[...], TN)
        slices = packed.shape[0]
        state_rows = state.shape[0] // slices
        packed[:, 0:state_rows, at : at + width] = state.astype(BF16).reshape(
            slices, state_rows, width
        )
        packed[:, state_rows:, at : at + width] = jnp.broadcast_to(
            jnp.exp(offset).astype(BF16)[None], (slices, E_ROWS, width)
        )


def local_state(kw, dw, vw, kn, dn, vn, slices):
    rows, keys_w = kw.shape
    keys_n = kn.shape[1]
    state_rows = vw.shape[1] // slices
    return pl.pallas_call(
        state_kernel,
        out_shape=jax.ShapeDtypeStruct((slices, state_rows + E_ROWS, keys_w + keys_n), BF16),
        scratch_shapes=[pltpu.VMEM((rows, keys_w), BF16), pltpu.VMEM((rows, keys_n), BF16)],
        compiler_params=params(),
        name="local_state",
    )(kw, dw, vw, kn, dn, vn)


def scan_kernel(packed, entering):
    slices, state_rows, width = entering.shape
    state = jnp.zeros((state_rows, width), F32)
    for i in range(slices):
        entering[i] = state.astype(BF16)
        if i + 1 < slices:
            decay = packed[i, state_rows : state_rows + 1, :].astype(F32)
            state = state * decay + packed[i, 0:state_rows, :].astype(F32)


def scan_states(packed):
    slices, packed_rows, width = packed.shape
    return pl.pallas_call(
        scan_kernel,
        out_shape=jax.ShapeDtypeStruct((slices, packed_rows - E_ROWS, width), BF16),
        compiler_params=params(),
        name="scan_states",
    )(packed)


def intra_kernel(q, k, v, pre, out, carried, memory, offset):
    @pl.when(pl.program_id(0) == 0)
    def _():
        memory[...] = jnp.zeros_like(memory)
        offset[...] = jnp.zeros_like(offset)

    width = q.shape[1]
    lower = tri_mask("lower")
    g = log_decay_of(pre[...])
    within = tri_sum(lower.astype(BF16), g)
    final = within[CHUNK - 1 : CHUNK, :]
    middle = within[CHUNK // 2 : CHUNK // 2 + 1, :]
    queries = q[...].astype(F32) * width ** (-0.5)
    keys = k[...].astype(F32)
    values = v[...]
    near_q = (queries * jnp.exp(within - middle)).astype(BF16)
    near_k = (keys * jnp.exp(middle - within)).astype(BF16)
    scores = jnp.where(lower, dot(near_q, near_k, NT), 0.0).astype(BF16)
    decayed_q = queries * jnp.exp(within)
    held = memory[...]
    outside = dot(decayed_q.astype(BF16), held.astype(BF16), NT)
    out[...] = outside + dot(scores, values)
    carried[...] = (decayed_q * jnp.exp(offset[...])).astype(BF16)
    offset[...] = offset[...] + final
    decayed_k = (keys * jnp.exp(final - within)).astype(BF16)
    memory[...] = held * jnp.exp(final) + dot(values, decayed_k, TN)


def intra(q, k, v, pre, name):
    rows, width = q.shape
    value_width = v.shape[1]

    def spec(cols):
        return pl.BlockSpec((CHUNK, cols), lambda i: (i, 0))

    return pl.pallas_call(
        intra_kernel,
        grid=(rows // CHUNK,),
        in_specs=[spec(width), spec(width), spec(value_width), spec(width)],
        out_specs=[spec(value_width), spec(width)],
        out_shape=[
            jax.ShapeDtypeStruct((rows, value_width), F32),
            jax.ShapeDtypeStruct((rows, width), BF16),
        ],
        scratch_shapes=[pltpu.VMEM((value_width, width), F32), pltpu.VMEM((1, width), F32)],
        compiler_params=params(dimension_semantics=("arbitrary",)),
        name=name,
    )(q, k, v, pre)


def project_kernel(aw, cw, gw, an, cn, gn, state, gain, ow, on, out):
    keys_w = cw.shape[1]

    def gated(inside, carried, gate, held):
        att = inside[...] + dot(carried[...], held, NT)
        scale = lax.rsqrt(jnp.mean(jnp.square(att), axis=-1, keepdims=True) + EPS)
        u = gate[...].astype(F32)
        return (att * scale * gain[...] * (u / (1.0 + jnp.exp(-u)))).astype(BF16)

    wide = gated(aw, cw, gw, state[:, :keys_w])
    narrow = gated(an, cn, gn, state[:, keys_w:])
    out[...] = (dot(wide, ow[...]) + dot(narrow, on[...])).astype(BF16)


def project(aw, cw, gw, an, cn, gn, state, gain, ow, on, blocks):
    rows = aw.shape[0]
    step = rows // blocks
    full = ow.shape[1]

    def spec(a):
        return pl.BlockSpec((step, a.shape[1]), lambda i: (i, 0))

    def whole(a):
        return pl.BlockSpec(a.shape, lambda i: (0, 0))

    return pl.pallas_call(
        project_kernel,
        grid=(blocks,),
        in_specs=[spec(a) for a in (aw, cw, gw, an, cn, gn)]
        + [whole(a) for a in (state, gain, ow, on)],
        out_specs=pl.BlockSpec((step, full), lambda i: (i, 0)),
        out_shape=jax.ShapeDtypeStruct((rows, full), BF16),
        compiler_params=params(dimension_semantics=("arbitrary",)),
        name="project",
    )(aw, cw, gw, an, cn, gn, state, gain, ow, on)


def stream_kernel(place, parts, residual, gain, stream, normed):
    total = residual[...].astype(F32)
    mixed = parts[0].astype(F32)
    for i in range(1, parts.shape[0]):
        mixed = mixed + parts[i].astype(F32)
    held = (total + mixed).astype(BF16)
    stream[...] = held
    wide = held.astype(F32)
    scale = lax.rsqrt(jnp.mean(jnp.square(wide), axis=-1, keepdims=True) + EPS)
    normed[...] = (wide * scale * gain[...]).astype(BF16)


def make_stream(place, parts, residual, gain):
    count, rows, full = parts.shape
    return pl.pallas_call(
        stream_kernel,
        grid_spec=pltpu.PrefetchScalarGridSpec(
            num_scalar_prefetch=1,
            grid=(1,),
            in_specs=[
                pl.BlockSpec((count, rows, full), lambda i, p: (0, 0, 0)),
                pl.BlockSpec((rows, full), lambda i, p: (p[0], 0)),
                pl.BlockSpec((1, full), lambda i, p: (0, 0)),
            ],
            out_specs=[
                pl.BlockSpec((rows, full), lambda i, p: (0, 0)),
                pl.BlockSpec((rows, full), lambda i, p: (0, 0)),
            ],
        ),
        out_shape=[jax.ShapeDtypeStruct((rows, full), BF16)] * 2,
        compiler_params=params(dimension_semantics=("arbitrary",)),
        name="make_stream",
    )(place, parts, residual, gain)


def mixer_kernel(normed, stream, up, down, out, total):
    step = pl.program_id(0)
    full = normed.shape[1]
    width = up.shape[-1]
    before = dot(normed[...], up[...].reshape(full, width))
    hidden = jnp.square(jnp.maximum(before, 0.0)).astype(BF16)
    term = dot(hidden, down[...].reshape(full, width), NT)

    @pl.when(step == 0)
    def _():
        total[...] = term

    @pl.when(step > 0)
    def _():
        total[...] = total[...] + term

    @pl.when(step == pl.num_programs(0) - 1)
    def _():
        cols = out.shape[2]
        for i in range(out.shape[0]):
            span = slice(i * cols, (i + 1) * cols)
            out[i] = (stream[:, span].astype(F32) + total[:, span]).astype(BF16)


def mixer(normed, stream, weights, count, width):
    rows, full = normed.shape
    n_sp, n_tp, both, cols = weights.shape
    per = cols // width

    def at(half):
        return pl.BlockSpec(
            (n_sp, 1, both // 2, width), lambda s: (0, s // per, half, s % per)
        )

    return pl.pallas_call(
        mixer_kernel,
        grid=(n_tp * per,),
        in_specs=[
            pl.BlockSpec((rows, full), lambda s: (0, 0)),
            pl.BlockSpec((rows, full), lambda s: (0, 0)),
            at(0),
            at(1),
        ],
        out_specs=pl.BlockSpec((count, rows, full // count), lambda s: (0, 0, 0)),
        out_shape=jax.ShapeDtypeStruct((count, rows, full // count), BF16),
        scratch_shapes=[pltpu.VMEM((rows, full), F32)],
        compiler_params=params(dimension_semantics=("arbitrary",)),
        name="mixer",
    )(normed, stream, weights, weights)


def body(
    residual,
    query_wide,
    key_wide,
    value_wide,
    decay_wide,
    gate_wide,
    query_narrow,
    key_narrow,
    value_narrow,
    decay_narrow,
    gate_narrow,
    head_gain,
    out_wide,
    out_narrow,
    mlp_gain,
    up_weight,
    down_weight,
):
    n_sp = lax.axis_size("sp")
    n_tp = lax.axis_size("tp")
    rows, full = residual.shape
    own = jnp.concatenate((up_weight, down_weight.T), axis=0)
    weights = lax.all_gather(own, ("sp", "tp"), axis=0, tiled=False)
    weights = weights.reshape(n_sp, n_tp, *own.shape)
    packed = local_state(
        key_wide, decay_wide, value_wide, key_narrow, decay_narrow, value_narrow, n_sp
    )
    packed = lax.all_to_all(packed, "sp", 0, 0, tiled=True)
    wide_in, wide_q = intra(query_wide, key_wide, value_wide, decay_wide, "intra_wide")
    narrow_in, narrow_q = intra(
        query_narrow, key_narrow, value_narrow, decay_narrow, "intra_narrow"
    )
    entering = lax.all_to_all(scan_states(packed), "sp", 0, 0, tiled=True)
    state = entering.reshape(-1, entering.shape[2])
    terms = project(
        wide_in,
        wide_q,
        gate_wide,
        narrow_in,
        narrow_q,
        gate_narrow,
        state,
        head_gain.reshape(1, -1),
        out_wide,
        out_narrow,
        n_tp,
    )
    parts = lax.all_to_all(terms.reshape(n_tp, rows // n_tp, full), "tp", 0, 0, tiled=True)
    place = lax.axis_index("tp").astype(jnp.int32).reshape(1)
    stream, normed = make_stream(place, parts, residual, mlp_gain.reshape(1, -1))
    finished = mixer(normed, stream, weights, n_tp, 512)
    sent = lax.all_to_all(finished, "tp", 0, 0, tiled=True)
    return sent.reshape(rows, full // n_tp)


def solution(mesh):
    return jax.shard_map(
        body,
        mesh=mesh,
        in_specs=(
            P("sp", None),
            P("sp", "tp"),
            P("sp", "tp"),
            P("sp", "tp"),
            P("sp", "tp"),
            P("sp", "tp"),
            P("sp", "tp"),
            P("sp", "tp"),
            P("sp", "tp"),
            P("sp", "tp"),
            P("sp", "tp"),
            P(),
            P("tp", None),
            P("tp", None),
            P(),
            P("sp", "tp"),
            P("tp", "sp"),
        ),
        out_specs=P("sp", "tp"),
        check_vma=False,
    )
```

```python
import jax
import jax.numpy as jnp
from jax import lax
from jax.experimental import pallas as pl
from jax.experimental.pallas import tpu as pltpu
from jax.sharding import Mesh, PartitionSpec as P

EPS = 1e-05
DECAY_NORMALIZER = 16.0
CHUNK = 128
F32 = jnp.float32
BF16 = jnp.bfloat16
NT = (((1,), (1,)), ((), ()))
TN = (((0,), (0,)), ((), ()))
E_ROWS = 8


def dot(a, b, dims=(((1,), (0,)), ((), ()))):
    return lax.dot_general(a, b, dims, preferred_element_type=F32)


def log_decay_of(pre):
    x = pre.astype(F32)
    return (jnp.minimum(x, 0.0) - jnp.log1p(jnp.exp(-jnp.abs(x)))) / DECAY_NORMALIZER


def tri_sum(tri, g):
    high = g.astype(BF16)
    low = (g - high.astype(F32)).astype(BF16)
    return dot(tri, high) + dot(tri, low)


def tri_mask(kind):
    row = lax.broadcasted_iota(jnp.int32, (CHUNK, CHUNK), 0)
    col = lax.broadcasted_iota(jnp.int32, (CHUNK, CHUNK), 1)
    return (col <= row) if kind == "lower" else (col > row)


def params(**kw):
    return pltpu.CompilerParams(vmem_limit_bytes=56 * 1024 * 1024, **kw)


def state_kernel(kw, dw, vw, kn, dn, vn, packed, decayed_w, decayed_n):
    later = tri_mask("upper").astype(BF16)
    rows = kw.shape[0]
    keys_w = kw.shape[1]
    for key, pre, decayed, value, at in (
        (kw, dw, decayed_w, vw, 0),
        (kn, dn, decayed_n, vn, keys_w),
    ):
        width = key.shape[1]
        offset = jnp.zeros((1, width), F32)
        for block in reversed(range(rows // CHUNK)):
            span = pl.ds(block * CHUNK, CHUNK)
            g = log_decay_of(pre[span, :])
            after = tri_sum(later, g)
            decayed[span, :] = (key[span, :].astype(F32) * jnp.exp(after + offset)).astype(BF16)
            offset = offset + after[0:1, :] + g[0:1, :]
        state = dot(value[...], decayed[...], TN)
        slices = packed.shape[0]
        state_rows = state.shape[0] // slices
        packed[:, 0:state_rows, at : at + width] = state.astype(BF16).reshape(
            slices, state_rows, width
        )
        packed[:, state_rows:, at : at + width] = jnp.broadcast_to(
            jnp.exp(offset).astype(BF16)[None], (slices, E_ROWS, width)
        )


def local_state(kw, dw, vw, kn, dn, vn, slices):
    rows, keys_w = kw.shape
    keys_n = kn.shape[1]
    state_rows = vw.shape[1] // slices
    return pl.pallas_call(
        state_kernel,
        out_shape=jax.ShapeDtypeStruct((slices, state_rows + E_ROWS, keys_w + keys_n), BF16),
        scratch_shapes=[pltpu.VMEM((rows, keys_w), BF16), pltpu.VMEM((rows, keys_n), BF16)],
        compiler_params=params(),
        name="local_state",
    )(kw, dw, vw, kn, dn, vn)


def scan_kernel(packed, after, entering):
    slices, state_rows, width = entering.shape
    state = jnp.zeros((state_rows, width), F32)
    for i in range(slices):
        entering[i] = state.astype(BF16)
        if i + 1 < slices:
            decay = packed[i, state_rows : state_rows + 1, :].astype(F32)
            state = state * decay + packed[i, 0:state_rows, :].astype(F32)


def scan_states(packed, after):
    slices, packed_rows, width = packed.shape
    return pl.pallas_call(
        scan_kernel,
        out_shape=jax.ShapeDtypeStruct((slices, packed_rows - E_ROWS, width), BF16),
        in_specs=[pl.BlockSpec(memory_space=pltpu.VMEM), pl.BlockSpec(memory_space=pl.ANY)],
        compiler_params=params(),
        name="scan_states",
    )(packed, after)


def intra_kernel(q, k, v, pre, out, carried, memory, offset):
    @pl.when(pl.program_id(0) == 0)
    def _():
        memory[...] = jnp.zeros_like(memory)
        offset[...] = jnp.zeros_like(offset)

    width = q.shape[1]
    lower = tri_mask("lower")
    g = log_decay_of(pre[...])
    within = tri_sum(lower.astype(BF16), g)
    final = within[CHUNK - 1 : CHUNK, :]
    middle = within[CHUNK // 2 : CHUNK // 2 + 1, :]
    queries = q[...].astype(F32) * width ** (-0.5)
    keys = k[...].astype(F32)
    values = v[...]
    near_q = (queries * jnp.exp(within - middle)).astype(BF16)
    near_k = (keys * jnp.exp(middle - within)).astype(BF16)
    scores = jnp.where(lower, dot(near_q, near_k, NT), 0.0).astype(BF16)
    decayed_q = queries * jnp.exp(within)
    held = memory[...]
    outside = dot(decayed_q.astype(BF16), held.astype(BF16), NT)
    out[...] = outside + dot(scores, values)
    carried[...] = (decayed_q * jnp.exp(offset[...])).astype(BF16)
    offset[...] = offset[...] + final
    decayed_k = (keys * jnp.exp(final - within)).astype(BF16)
    memory[...] = held * jnp.exp(final) + dot(values, decayed_k, TN)


def intra(q, k, v, pre, name):
    rows, width = q.shape
    value_width = v.shape[1]

    def spec(cols):
        return pl.BlockSpec((CHUNK, cols), lambda i: (i, 0))

    return pl.pallas_call(
        intra_kernel,
        grid=(rows // CHUNK,),
        in_specs=[spec(width), spec(width), spec(value_width), spec(width)],
        out_specs=[spec(value_width), spec(width)],
        out_shape=[
            jax.ShapeDtypeStruct((rows, value_width), F32),
            jax.ShapeDtypeStruct((rows, width), BF16),
        ],
        scratch_shapes=[pltpu.VMEM((value_width, width), F32), pltpu.VMEM((1, width), F32)],
        compiler_params=params(dimension_semantics=("arbitrary",)),
        name=name,
    )(q, k, v, pre)


def gated_of(inside, carried, gate, held, gain):
    att = inside[...] + dot(carried[...], held, NT)
    scale = lax.rsqrt(jnp.mean(jnp.square(att), axis=-1, keepdims=True) + EPS)
    u = gate[...].astype(F32)
    return (att * scale * gain[...] * (u / (1.0 + jnp.exp(-u)))).astype(BF16)


def project_kernel(place, aw, cw, gw, an, cn, gn, state, gain, ow, on, *outs):
    keys_w = cw.shape[1]
    wide = gated_of(aw, cw, gw, state[:, :keys_w], gain)
    narrow = gated_of(an, cn, gn, state[:, keys_w:], gain)
    term = dot(wide, ow[...]) + dot(narrow, on[...])
    half = term.shape[0] // 2
    step = pl.program_id(0)
    if len(outs) == 2:
        outs[0][...] = term[:half].astype(BF16)
        outs[1][...] = term[half:].astype(BF16)
        return

    @pl.when(step == 0)
    def _():
        outs[0][...] = term[:half].astype(BF16)
        outs[1][...] = term[half:].astype(BF16)

    @pl.when(step == 1)
    def _():
        outs[2][...] = term[:half].astype(BF16)
        outs[3][...] = term[half:].astype(BF16)

    @pl.when(step == 2)
    def _():
        outs[4][...] = term


def project(place, arrays, state, gain, ow, on, blocks, turns, name):
    rows = arrays[0].shape[0]
    step = rows // blocks
    full = ow.shape[1]

    def block_of(i, p):
        turn = turns[0]
        for n in range(1, len(turns)):
            turn = jnp.where(i == n, turns[n], turn)
        return lax.rem(p[0] + turn, blocks)

    def spec(a):
        return pl.BlockSpec((step, a.shape[1]), lambda i, p: (block_of(i, p), 0))

    def whole(a):
        return pl.BlockSpec(a.shape, lambda i, p: (0, 0))

    half = jax.ShapeDtypeStruct((step // 2, full), BF16)
    shapes = [half, half]
    if len(turns) > 1:
        shapes = [half] * 4 + [jax.ShapeDtypeStruct((step, full), F32)]
    return pl.pallas_call(
        project_kernel,
        grid_spec=pltpu.PrefetchScalarGridSpec(
            num_scalar_prefetch=1,
            grid=(len(turns),),
            in_specs=[spec(a) for a in arrays] + [whole(a) for a in (state, gain, ow, on)],
            out_specs=[whole(o) for o in shapes],
        ),
        out_shape=shapes,
        compiler_params=params(dimension_semantics=("arbitrary",)),
        name=name,
    )(place, *arrays, state, gain, ow, on)


def add_kernel(a, b, c, d, first, second):
    first[...] = (a[...].astype(F32) + b[...].astype(F32)).astype(BF16)
    second[...] = (c[...].astype(F32) + d[...].astype(F32)).astype(BF16)


def add_pairs(a, b, c, d):
    shape = jax.ShapeDtypeStruct(a.shape, BF16)
    return pl.pallas_call(
        add_kernel, out_shape=[shape, shape], compiler_params=params(), name="add_pairs"
    )(a, b, c, d)


def stream_kernel(place, own, prev_low, prev_high, next_low, next_high, residual, gain, stream, normed):
    half = prev_low.shape[0]
    for at, first, second in ((0, prev_low, next_low), (half, prev_high, next_high)):
        span = slice(at, at + half)
        mixed = own[span, :] + first[...].astype(F32) + second[...].astype(F32)
        held = (residual[span, :].astype(F32) + mixed).astype(BF16)
        stream[span, :] = held
        wide = held.astype(F32)
        scale = lax.rsqrt(jnp.mean(jnp.square(wide), axis=-1, keepdims=True) + EPS)
        normed[span, :] = (wide * scale * gain[...]).astype(BF16)


def make_stream(place, own, pieces, residual, gain):
    rows, full = own.shape

    def whole(a):
        return pl.BlockSpec(a.shape, lambda i, p: (0, 0))

    return pl.pallas_call(
        stream_kernel,
        grid_spec=pltpu.PrefetchScalarGridSpec(
            num_scalar_prefetch=1,
            grid=(1,),
            in_specs=[
                whole(own),
                *[whole(a) for a in pieces],
                pl.BlockSpec((rows, full), lambda i, p: (p[0], 0)),
                whole(gain),
            ],
            out_specs=[pl.BlockSpec((rows, full), lambda i, p: (0, 0))] * 2,
        ),
        out_shape=[jax.ShapeDtypeStruct((rows, full), BF16)] * 2,
        compiler_params=params(dimension_semantics=("arbitrary",)),
        name="make_stream",
    )(place, own, *pieces, residual, gain)


def mixer_kernel(place, normed, stream, weights, *refs):
    *outs, held_up, held_down, hidden, up_sems, down_sems = refs
    count, n_sp, each, width = held_up.shape
    blocks, per_block, n_x, _, cols = held_down.shape
    per = cols // width
    full = normed.shape[1]
    block_cols = per_block * each
    ups, downs = [], []
    for s in range(count):
        source = weights.at[:, s // per, 0:each, pl.ds((s % per) * width, width)]
        ups.append(pltpu.make_async_copy(source, held_up.at[s], up_sems.at[s]))
    turns = (2, 1, 3, 0)
    for b, turn in enumerate(turns):
        block = lax.rem(place[0] + turn, blocks)
        source = weights.at[pl.ds(block * per_block, per_block), :, each : 2 * each, :]
        downs.append(pltpu.make_async_copy(source, held_down.at[b], down_sems.at[b]))
    for copy in ups + downs:
        copy.start()
    for s in range(count):
        ups[s].wait()
        before = dot(normed[...], held_up[s].reshape(full, width))
        hidden[:, s * width : (s + 1) * width] = jnp.square(jnp.maximum(before, 0.0)).astype(BF16)
    for b, turn in enumerate(turns):
        downs[b].wait()
        block = lax.rem(place[0] + turn, blocks)
        start = pl.multiple_of(block * block_cols, block_cols)
        total = stream[:, pl.ds(start, block_cols)].astype(F32)
        for x in range(n_x):
            total = total + dot(
                hidden[:, x * cols : (x + 1) * cols],
                held_down[b, :, x].reshape(block_cols, cols),
                NT,
            )
        outs[b][...] = total.astype(BF16)


def mixer(place, normed, stream, weights, count, width):
    rows, full = normed.shape
    n_sp, n_x, both, cols = weights.shape
    each = both // 2
    steps = n_x * cols // width
    vmem = pl.BlockSpec(memory_space=pltpu.VMEM)
    return pl.pallas_call(
        mixer_kernel,
        in_specs=[
            pl.BlockSpec(memory_space=pltpu.SMEM),
            vmem,
            vmem,
            pl.BlockSpec(memory_space=pl.ANY),
        ],
        out_shape=[jax.ShapeDtypeStruct((rows, full // count), BF16)] * count,
        scratch_shapes=[
            pltpu.VMEM((steps, n_sp, each, width), BF16),
            pltpu.VMEM((count, n_sp // count, n_x, each, cols), BF16),
            pltpu.VMEM((rows, n_x * cols), BF16),
            pltpu.SemaphoreType.DMA((steps,)),
            pltpu.SemaphoreType.DMA((count,)),
        ],
        compiler_params=pltpu.CompilerParams(vmem_limit_bytes=60 * 1024 * 1024),
        name="mixer",
    )(place, normed, stream, weights)


def rows_kernel(place, *refs):
    *pieces, out = refs
    rows = pieces[0].shape[0]
    for r, piece in enumerate(pieces):
        block = lax.rem(place[0] - r + len(pieces), len(pieces))
        out[pl.ds(pl.multiple_of(block * rows, rows), rows), :] = piece[...]


def gather_rows(place, pieces):
    rows, cols = pieces[0].shape
    return pl.pallas_call(
        rows_kernel,
        in_specs=[pl.BlockSpec(memory_space=pltpu.SMEM)]
        + [pl.BlockSpec(memory_space=pltpu.VMEM)] * len(pieces),
        out_shape=jax.ShapeDtypeStruct((len(pieces) * rows, cols), BF16),
        compiler_params=params(),
        name="gather_rows",
    )(place, *pieces)


def shifted(array, axis, step):
    count = lax.axis_size(axis)
    return lax.ppermute(array, axis, [(i, (i + step) % count) for i in range(count)])


def held_until(arrays, *others):
    return list(lax.optimization_barrier((tuple(arrays), others))[0])


def body(
    residual,
    query_wide,
    key_wide,
    value_wide,
    decay_wide,
    gate_wide,
    query_narrow,
    key_narrow,
    value_narrow,
    decay_narrow,
    gate_narrow,
    head_gain,
    out_wide,
    out_narrow,
    mlp_gain,
    up_weight,
    down_weight,
):
    n_x = lax.axis_size("x")
    line = ("z", "y", "c")
    n_sp = lax.axis_size(line)
    rows, full = residual.shape
    place = lax.axis_index("x").astype(jnp.int32).reshape(1)
    own = jnp.concatenate((up_weight, down_weight.T), axis=0)
    weights = lax.all_gather(own, (*line, "x"), axis=0, tiled=False)
    weights = weights.reshape(n_sp, n_x, *own.shape)
    packed = local_state(
        key_wide, decay_wide, value_wide, key_narrow, decay_narrow, value_narrow, n_sp
    )
    received = lax.all_to_all(packed, line, 0, 0, tiled=True)
    wide_in, wide_q = intra(query_wide, key_wide, value_wide, decay_wide, "intra_wide")
    entering = scan_states(received, wide_q)
    arrived = lax.all_to_all(entering, line, 0, 0, tiled=True)
    (query_narrow,) = held_until([query_narrow], entering)
    narrow_in, narrow_q = intra(
        query_narrow, key_narrow, value_narrow, decay_narrow, "intra_narrow"
    )
    (arrived,) = held_until([arrived], narrow_q)
    state = arrived.reshape(-1, arrived.shape[2])
    arrays = (wide_in, wide_q, gate_wide, narrow_in, narrow_q, gate_narrow)
    rest = (state, head_gain.reshape(1, -1), out_wide, out_narrow, n_x)
    far_low, far_high = project(place, arrays, *rest, (2,), "project_far")
    from_prev = shifted(far_low, "x", 1)
    from_next = shifted(far_high, "x", -1)
    next_low, next_high, prev_low, prev_high, own = project(
        place, arrays, *rest, (1, 3, 0), "project_near"
    )
    high_of_prev = shifted(next_high, "x", 1)
    low_of_next = shifted(prev_low, "x", -1)
    next_low, prev_high = add_pairs(next_low, from_prev, prev_high, from_next)
    low_of_prev = shifted(next_low, "x", 1)
    high_of_next = shifted(prev_high, "x", -1)
    stream, normed = make_stream(
        place,
        own,
        (low_of_prev, high_of_prev, low_of_next, high_of_next),
        residual,
        mlp_gain.reshape(1, -1),
    )
    opposite, after, before, kept = mixer(place, normed, stream, weights, n_x, 512)
    opposite = shifted(opposite, "x", 2)
    after = shifted(after, "x", 1)
    before = shifted(before, "x", -1)
    return gather_rows(place, (kept, after, opposite, before))


def solution(mesh):
    n_tp = mesh.shape["tp"]
    side = int(round((mesh.shape["sp"] // 2) ** 0.5))
    cut = Mesh(mesh.devices.reshape(side, side, 2, n_tp), ("z", "y", "c", "x"))
    line = ("z", "y", "c")
    step = jax.shard_map(
        body,
        mesh=cut,
        in_specs=(
            P(line, None),
            P(line, "x"),
            P(line, "x"),
            P(line, "x"),
            P(line, "x"),
            P(line, "x"),
            P(line, "x"),
            P(line, "x"),
            P(line, "x"),
            P(line, "x"),
            P(line, "x"),
            P(),
            P("x", None),
            P("x", None),
            P(),
            P(line, "x"),
            P("x", line),
        ),
        out_specs=P(line, "x"),
        check_vma=False,
    )
    return step
```

```python
import jax
import jax.numpy as jnp
from jax import lax
from jax.experimental import pallas as pl
from jax.experimental.pallas import tpu as pltpu
from jax.sharding import Mesh, PartitionSpec as P

EPS = 1e-05
DECAY_NORMALIZER = 16.0
CHUNK = 128
F32 = jnp.float32
BF16 = jnp.bfloat16
NT = (((1,), (1,)), ((), ()))
TN = (((0,), (0,)), ((), ()))
E_ROWS = 8
WIDE = 58


def dot(a, b, dims=(((1,), (0,)), ((), ()))):
    return lax.dot_general(a, b, dims, preferred_element_type=F32)


def log_decay_of(pre):
    x = pre.astype(F32)
    return (jnp.minimum(x, 0.0) - jnp.log1p(jnp.exp(-jnp.abs(x)))) / DECAY_NORMALIZER


def tri_sum(tri, g):
    high = g.astype(BF16)
    low = (g - high.astype(F32)).astype(BF16)
    return dot(tri, high) + dot(tri, low)


def tri_mask(kind):
    row = lax.broadcasted_iota(jnp.int32, (CHUNK, CHUNK), 0)
    col = lax.broadcasted_iota(jnp.int32, (CHUNK, CHUNK), 1)
    return (col <= row) if kind == "lower" else (col > row)


def params(mib=24, **kw):
    return pltpu.CompilerParams(vmem_limit_bytes=mib * 1024 * 1024, **kw)


def state_kernel(kw, dw, vw, kn, dn, vn, packed, decayed_w, decayed_n):
    later = tri_mask("upper").astype(BF16)
    rows = kw.shape[0]
    keys_w = kw.shape[1]
    for key, pre, decayed, value, at in (
        (kw, dw, decayed_w, vw, 0),
        (kn, dn, decayed_n, vn, keys_w),
    ):
        width = key.shape[1]
        offset = jnp.zeros((1, width), F32)
        for block in reversed(range(rows // CHUNK)):
            span = pl.ds(block * CHUNK, CHUNK)
            g = log_decay_of(pre[span, :])
            after = tri_sum(later, g)
            decayed[span, :] = (key[span, :].astype(F32) * jnp.exp(after + offset)).astype(BF16)
            offset = offset + after[0:1, :] + g[0:1, :]
        state = dot(value[...], decayed[...], TN)
        slices = packed.shape[0]
        state_rows = state.shape[0] // slices
        packed[:, 0:state_rows, at : at + width] = state.astype(BF16).reshape(
            slices, state_rows, width
        )
        packed[:, state_rows:, at : at + width] = jnp.broadcast_to(
            jnp.exp(offset).astype(BF16)[None], (slices, E_ROWS, width)
        )


def local_state(kw, dw, vw, kn, dn, vn, slices):
    rows, keys_w = kw.shape
    keys_n = kn.shape[1]
    state_rows = vw.shape[1] // slices
    return pl.pallas_call(
        state_kernel,
        out_shape=jax.ShapeDtypeStruct((slices, state_rows + E_ROWS, keys_w + keys_n), BF16),
        scratch_shapes=[pltpu.VMEM((rows, keys_w), BF16), pltpu.VMEM((rows, keys_n), BF16)],
        compiler_params=params(WIDE),
        name="local_state",
    )(kw, dw, vw, kn, dn, vn)


def scan_kernel(packed, after, entering):
    slices, state_rows, width = entering.shape
    state = jnp.zeros((state_rows, width), F32)
    for i in range(slices):
        entering[i] = state.astype(BF16)
        if i + 1 < slices:
            decay = packed[i, state_rows : state_rows + 1, :].astype(F32)
            state = state * decay + packed[i, 0:state_rows, :].astype(F32)


def scan_states(packed, after):
    slices, packed_rows, width = packed.shape
    return pl.pallas_call(
        scan_kernel,
        out_shape=jax.ShapeDtypeStruct((slices, packed_rows - E_ROWS, width), BF16),
        in_specs=[pl.BlockSpec(memory_space=pltpu.VMEM), pl.BlockSpec(memory_space=pl.ANY)],
        compiler_params=params(),
        name="scan_states",
    )(packed, after)


def intra_kernel(q, k, v, pre, out, carried, memory, offset):
    @pl.when(pl.program_id(0) == 0)
    def _():
        memory[...] = jnp.zeros_like(memory)
        offset[...] = jnp.zeros_like(offset)

    width = q.shape[1]
    lower = tri_mask("lower")
    g = log_decay_of(pre[...])
    within = tri_sum(lower.astype(BF16), g)
    final = within[CHUNK - 1 : CHUNK, :]
    middle = within[CHUNK // 2 : CHUNK // 2 + 1, :]
    queries = q[...].astype(F32) * width ** (-0.5)
    keys = k[...].astype(F32)
    values = v[...]
    near_q = (queries * jnp.exp(within - middle)).astype(BF16)
    near_k = (keys * jnp.exp(middle - within)).astype(BF16)
    scores = jnp.where(lower, dot(near_q, near_k, NT), 0.0).astype(BF16)
    decayed_q = queries * jnp.exp(within)
    held = memory[...]
    outside = dot(decayed_q.astype(BF16), held.astype(BF16), NT)
    out[...] = (outside + dot(scores, values)).astype(BF16)
    carried[...] = (decayed_q * jnp.exp(offset[...])).astype(BF16)
    offset[...] = offset[...] + final
    decayed_k = (keys * jnp.exp(final - within)).astype(BF16)
    memory[...] = held * jnp.exp(final) + dot(values, decayed_k, TN)


def intra(q, k, v, pre, name):
    rows, width = q.shape
    value_width = v.shape[1]

    def spec(cols):
        return pl.BlockSpec((CHUNK, cols), lambda i: (i, 0))

    return pl.pallas_call(
        intra_kernel,
        grid=(rows // CHUNK,),
        in_specs=[spec(width), spec(width), spec(value_width), spec(width)],
        out_specs=[spec(value_width), spec(width)],
        out_shape=[
            jax.ShapeDtypeStruct((rows, value_width), BF16),
            jax.ShapeDtypeStruct((rows, width), BF16),
        ],
        scratch_shapes=[pltpu.VMEM((value_width, width), F32), pltpu.VMEM((1, width), F32)],
        compiler_params=params(WIDE, dimension_semantics=("arbitrary",)),
        name=name,
    )(q, k, v, pre)


def gated_of(inside, carried, gate, held, gain):
    att = inside[...].astype(F32) + dot(carried[...], held, NT)
    scale = lax.rsqrt(jnp.mean(jnp.square(att), axis=-1, keepdims=True) + EPS)
    u = gate[...].astype(F32)
    return (att * scale * gain[...] * (u / (1.0 + jnp.exp(-u)))).astype(BF16)


def project_kernel(place, aw, cw, gw, an, cn, gn, state, gain, ow, on, *outs):
    keys_w = cw.shape[1]
    wide = gated_of(aw, cw, gw, state[:, :keys_w], gain)
    narrow = gated_of(an, cn, gn, state[:, keys_w:], gain)
    term = dot(wide, ow[...]) + dot(narrow, on[...])
    half = term.shape[0] // 2
    step = pl.program_id(0)
    if len(outs) == 2:
        outs[0][...] = term[:half].astype(BF16)
        outs[1][...] = term[half:].astype(BF16)
        return

    @pl.when(step == 0)
    def _():
        outs[0][...] = term[:half].astype(BF16)
        outs[1][...] = term[half:].astype(BF16)

    @pl.when(step == 1)
    def _():
        outs[2][...] = term[:half].astype(BF16)
        outs[3][...] = term[half:].astype(BF16)

    @pl.when(step == 2)
    def _():
        outs[4][...] = term


def project(place, arrays, state, gain, ow, on, blocks, turns, name):
    rows = arrays[0].shape[0]
    step = rows // blocks
    full = ow.shape[1]

    def block_of(i, p):
        turn = turns[0]
        for n in range(1, len(turns)):
            turn = jnp.where(i == n, turns[n], turn)
        return lax.rem(p[0] + turn, blocks)

    def spec(a):
        return pl.BlockSpec((step, a.shape[1]), lambda i, p: (block_of(i, p), 0))

    def whole(a):
        return pl.BlockSpec(a.shape, lambda i, p: (0, 0))

    half = jax.ShapeDtypeStruct((step // 2, full), BF16)
    shapes = [half, half]
    if len(turns) > 1:
        shapes = [half] * 4 + [jax.ShapeDtypeStruct((step, full), F32)]
    return pl.pallas_call(
        project_kernel,
        grid_spec=pltpu.PrefetchScalarGridSpec(
            num_scalar_prefetch=1,
            grid=(len(turns),),
            in_specs=[spec(a) for a in arrays] + [whole(a) for a in (state, gain, ow, on)],
            out_specs=[whole(o) for o in shapes],
        ),
        out_shape=shapes,
        compiler_params=params(dimension_semantics=("arbitrary",)),
        name=name,
    )(place, *arrays, state, gain, ow, on)


def add_kernel(a, b, c, d, first, second):
    first[...] = (a[...].astype(F32) + b[...].astype(F32)).astype(BF16)
    second[...] = (c[...].astype(F32) + d[...].astype(F32)).astype(BF16)


def add_pairs(a, b, c, d):
    shape = jax.ShapeDtypeStruct(a.shape, BF16)
    return pl.pallas_call(
        add_kernel, out_shape=[shape, shape], compiler_params=params(), name="add_pairs"
    )(a, b, c, d)


def stream_kernel(place, own, prev_low, prev_high, next_low, next_high, residual, gain, stream, normed):
    half = prev_low.shape[0]
    for at, first, second in ((0, prev_low, next_low), (half, prev_high, next_high)):
        span = slice(at, at + half)
        mixed = own[span, :] + first[...].astype(F32) + second[...].astype(F32)
        held = (residual[span, :].astype(F32) + mixed).astype(BF16)
        stream[span, :] = held
        wide = held.astype(F32)
        scale = lax.rsqrt(jnp.mean(jnp.square(wide), axis=-1, keepdims=True) + EPS)
        normed[span, :] = (wide * scale * gain[...]).astype(BF16)


def make_stream(place, own, pieces, residual, gain):
    rows, full = own.shape

    def whole(a):
        return pl.BlockSpec(a.shape, lambda i, p: (0, 0))

    return pl.pallas_call(
        stream_kernel,
        grid_spec=pltpu.PrefetchScalarGridSpec(
            num_scalar_prefetch=1,
            grid=(1,),
            in_specs=[
                whole(own),
                *[whole(a) for a in pieces],
                pl.BlockSpec((rows, full), lambda i, p: (p[0], 0)),
                whole(gain),
            ],
            out_specs=[pl.BlockSpec((rows, full), lambda i, p: (0, 0))] * 2,
        ),
        out_shape=[jax.ShapeDtypeStruct((rows, full), BF16)] * 2,
        compiler_params=params(dimension_semantics=("arbitrary",)),
        name="make_stream",
    )(place, own, *pieces, residual, gain)


def mixer_kernel(place, normed, stream, weights, *refs):
    *outs, held_up, held_down, hidden, up_sems, down_sems = refs
    count, n_sp, each, width = held_up.shape
    blocks, per_block, n_x, _, cols = held_down.shape
    per = cols // width
    full = normed.shape[1]
    block_cols = per_block * each
    ups, downs = [], []
    for s in range(count):
        source = weights.at[:, s // per, 0:each, pl.ds((s % per) * width, width)]
        ups.append(pltpu.make_async_copy(source, held_up.at[s], up_sems.at[s]))
    turns = (2, 1, 3, 0)
    for b, turn in enumerate(turns):
        block = lax.rem(place[0] + turn, blocks)
        source = weights.at[pl.ds(block * per_block, per_block), :, each : 2 * each, :]
        downs.append(pltpu.make_async_copy(source, held_down.at[b], down_sems.at[b]))
    for copy in ups + downs:
        copy.start()
    for s in range(count):
        ups[s].wait()
        before = dot(normed[...], held_up[s].reshape(full, width))
        hidden[:, s * width : (s + 1) * width] = jnp.square(jnp.maximum(before, 0.0)).astype(BF16)
    for b, turn in enumerate(turns):
        downs[b].wait()
        block = lax.rem(place[0] + turn, blocks)
        start = pl.multiple_of(block * block_cols, block_cols)
        total = stream[:, pl.ds(start, block_cols)].astype(F32)
        for x in range(n_x):
            total = total + dot(
                hidden[:, x * cols : (x + 1) * cols],
                held_down[b, :, x].reshape(block_cols, cols),
                NT,
            )
        outs[b][...] = total.astype(BF16)


def mixer(place, normed, stream, weights, count, width):
    rows, full = normed.shape
    n_sp, n_x, both, cols = weights.shape
    each = both // 2
    steps = n_x * cols // width
    vmem = pl.BlockSpec(memory_space=pltpu.VMEM)
    return pl.pallas_call(
        mixer_kernel,
        in_specs=[
            pl.BlockSpec(memory_space=pltpu.SMEM),
            vmem,
            vmem,
            pl.BlockSpec(memory_space=pl.ANY),
        ],
        out_shape=[jax.ShapeDtypeStruct((rows, full // count), BF16)] * count,
        scratch_shapes=[
            pltpu.VMEM((steps, n_sp, each, width), BF16),
            pltpu.VMEM((count, n_sp // count, n_x, each, cols), BF16),
            pltpu.VMEM((rows, n_x * cols), BF16),
            pltpu.SemaphoreType.DMA((steps,)),
            pltpu.SemaphoreType.DMA((count,)),
        ],
        compiler_params=pltpu.CompilerParams(vmem_limit_bytes=60 * 1024 * 1024),
        name="mixer",
    )(place, normed, stream, weights)


def stacked_kernel(first, second, out):
    rows = first.shape[0]
    out[0:rows, :] = first[...]
    out[rows:, :] = second[...]


def stacked_rows(first, second):
    rows, cols = first.shape
    return pl.pallas_call(
        stacked_kernel,
        out_shape=jax.ShapeDtypeStruct((2 * rows, cols), BF16),
        compiler_params=params(WIDE),
        name="stacked_rows",
    )(first, second)


def rows_kernel(place, *refs):
    *pieces, out = refs
    rows = pieces[0].shape[0]
    for r, piece in enumerate(pieces):
        block = lax.rem(place[0] - r + len(pieces), len(pieces))
        out[pl.ds(pl.multiple_of(block * rows, rows), rows), :] = piece[...]


def gather_rows(place, pieces):
    rows, cols = pieces[0].shape
    return pl.pallas_call(
        rows_kernel,
        in_specs=[pl.BlockSpec(memory_space=pltpu.SMEM)]
        + [pl.BlockSpec(memory_space=pltpu.VMEM)] * len(pieces),
        out_shape=jax.ShapeDtypeStruct((len(pieces) * rows, cols), BF16),
        compiler_params=params(8),
        name="gather_rows",
    )(place, *pieces)


def shifted(array, axis, step):
    count = lax.axis_size(axis)
    return lax.ppermute(array, axis, [(i, (i + step) % count) for i in range(count)])


def near(array):
    return pltpu.with_memory_space_constraint(array, pltpu.VMEM)


def away(array):
    return pltpu.with_memory_space_constraint(array, pltpu.HBM)


def held_until(arrays, *others):
    return list(lax.optimization_barrier((tuple(arrays), others))[0])


def body(
    residual,
    query_wide,
    key_wide,
    value_wide,
    decay_wide,
    gate_wide,
    query_narrow,
    key_narrow,
    value_narrow,
    decay_narrow,
    gate_narrow,
    head_gain,
    out_wide,
    out_narrow,
    mlp_gain,
    up_weight,
    down_weight,
):
    n_x = lax.axis_size("x")
    line = ("z", "y", "c")
    n_sp = lax.axis_size(line)
    rows, full = residual.shape
    place = lax.axis_index("x").astype(jnp.int32).reshape(1)
    own = stacked_rows(up_weight, down_weight.T)
    weights = lax.all_gather(own, (*line, "x"), axis=0, tiled=False)
    weights = weights.reshape(n_sp, n_x, *own.shape)
    packed = local_state(
        key_wide, decay_wide, value_wide, key_narrow, decay_narrow, value_narrow, n_sp
    )
    received = lax.all_to_all(packed, line, 0, 0, tiled=True)
    wide_in, wide_q = intra(query_wide, key_wide, value_wide, decay_wide, "intra_wide")
    entering = scan_states(near(received), wide_q)
    arrived = lax.all_to_all(entering, line, 0, 0, tiled=True)
    (query_narrow,) = held_until([query_narrow], entering)
    narrow_in, narrow_q = intra(
        query_narrow, key_narrow, value_narrow, decay_narrow, "intra_narrow"
    )
    (arrived,) = held_until([arrived], narrow_q)
    state = near(arrived.reshape(-1, arrived.shape[2]))
    arrays = tuple(
        away(a) for a in (wide_in, wide_q, gate_wide, narrow_in, narrow_q, gate_narrow)
    )
    rest = (state, head_gain.reshape(1, -1), away(out_wide), away(out_narrow), n_x)
    far_low, far_high = project(place, arrays, *rest, (2,), "project_far")
    from_prev = shifted(far_low, "x", 1)
    from_next = shifted(far_high, "x", -1)
    next_low, next_high, prev_low, prev_high, own = project(
        place, arrays, *rest, (1, 3, 0), "project_near"
    )
    high_of_prev = shifted(next_high, "x", 1)
    low_of_next = shifted(prev_low, "x", -1)
    next_low, prev_high = add_pairs(next_low, near(from_prev), prev_high, near(from_next))
    low_of_prev = shifted(next_low, "x", 1)
    high_of_next = shifted(prev_high, "x", -1)
    stream, normed = make_stream(
        place,
        own,
        tuple(near(a) for a in (low_of_prev, high_of_prev, low_of_next, high_of_next)),
        away(residual),
        mlp_gain.reshape(1, -1),
    )
    opposite, after, before, kept = mixer(place, normed, stream, weights, n_x, 512)
    opposite = shifted(opposite, "x", 2)
    after = shifted(after, "x", 1)
    before = shifted(before, "x", -1)
    return gather_rows(place, (near(kept), near(after), near(opposite), near(before)))


def solution(mesh):
    n_tp = mesh.shape["tp"]
    side = int(round((mesh.shape["sp"] // 2) ** 0.5))
    cut = Mesh(mesh.devices.reshape(side, side, 2, n_tp), ("z", "y", "c", "x"))
    line = ("z", "y", "c")
    step = jax.shard_map(
        body,
        mesh=cut,
        in_specs=(
            P(line, None),
            P(line, "x"),
            P(line, "x"),
            P(line, "x"),
            P(line, "x"),
            P(line, "x"),
            P(line, "x"),
            P(line, "x"),
            P(line, "x"),
            P(line, "x"),
            P(line, "x"),
            P(),
            P("x", None),
            P("x", None),
            P(),
            P(line, "x"),
            P("x", line),
        ),
        out_specs=P(line, "x"),
        check_vma=False,
    )
    return step
```

```python
import jax
import jax.numpy as jnp
from jax import lax
from jax.experimental import pallas as pl
from jax.experimental.pallas import tpu as pltpu
from jax.sharding import Mesh, PartitionSpec as P

EPS = 1e-05
DECAY_NORMALIZER = 16.0
CHUNK = 128
F32 = jnp.float32
BF16 = jnp.bfloat16
NT = (((1,), (1,)), ((), ()))
TN = (((0,), (0,)), ((), ()))
LANES = 128
WIDE = 58


def dot(a, b, dims=(((1,), (0,)), ((), ()))):
    return lax.dot_general(a, b, dims, preferred_element_type=F32)


def log_decay_of(pre):
    x = pre.astype(F32)
    return (jnp.minimum(x, 0.0) - jnp.log1p(jnp.exp(-jnp.abs(x)))) / DECAY_NORMALIZER


def tri_sum(tri, g):
    high = g.astype(BF16)
    low = (g - high.astype(F32)).astype(BF16)
    return dot(tri, high) + dot(tri, low)


def tri_mask(kind):
    row = lax.broadcasted_iota(jnp.int32, (CHUNK, CHUNK), 0)
    col = lax.broadcasted_iota(jnp.int32, (CHUNK, CHUNK), 1)
    return (col <= row) if kind == "lower" else (col > row)


def params(mib=24, **kw):
    return pltpu.CompilerParams(vmem_limit_bytes=mib * 1024 * 1024, **kw)


def state_kernel(kw, dw, vw, kn, dn, vn, packed, decayed_w, decayed_n):
    later = tri_mask("upper").astype(BF16)
    rows = kw.shape[0]
    keys_w = kw.shape[1]
    for key, pre, decayed, value, at in (
        (kw, dw, decayed_w, vw, 0),
        (kn, dn, decayed_n, vn, keys_w),
    ):
        width = key.shape[1]
        offset = jnp.zeros((1, width), F32)
        for block in reversed(range(rows // CHUNK)):
            span = pl.ds(block * CHUNK, CHUNK)
            g = log_decay_of(pre[span, :])
            after = tri_sum(later, g)
            decayed[span, :] = (key[span, :].astype(F32) * jnp.exp(after + offset)).astype(BF16)
            offset = offset + after[0:1, :] + g[0:1, :]
        state = dot(value[...], decayed[...], TN)
        slices = packed.shape[0]
        state_rows = state.shape[0] // slices
        packed[:, :, at : at + width] = state.astype(BF16).reshape(slices, state_rows, width)
        decay = jnp.exp(offset).astype(BF16)
        for lane in range(0, width, LANES):
            row = (at + lane) // LANES
            packed[:, row : row + 1, -LANES:] = jnp.broadcast_to(
                decay[None, :, lane : lane + LANES], (slices, 1, LANES)
            )


def local_state(kw, dw, vw, kn, dn, vn, slices):
    rows, keys_w = kw.shape
    keys_n = kn.shape[1]
    state_rows = vw.shape[1] // slices
    return pl.pallas_call(
        state_kernel,
        out_shape=jax.ShapeDtypeStruct((slices, state_rows, keys_w + keys_n + LANES), BF16),
        scratch_shapes=[pltpu.VMEM((rows, keys_w), BF16), pltpu.VMEM((rows, keys_n), BF16)],
        compiler_params=params(WIDE),
        name="local_state",
    )(kw, dw, vw, kn, dn, vn)


def scan_kernel(packed, after, entering):
    slices, state_rows, width = entering.shape
    state = jnp.zeros((state_rows, width), F32)
    for i in range(slices):
        entering[i] = state.astype(BF16)
        if i + 1 < slices:
            decay = jnp.concatenate(
                [packed[i, r : r + 1, width:].astype(F32) for r in range(width // LANES)], axis=1
            )
            state = state * decay + packed[i, :, 0:width].astype(F32)


def scan_states(packed, after):
    slices, packed_rows, width = packed.shape
    return pl.pallas_call(
        scan_kernel,
        out_shape=jax.ShapeDtypeStruct((slices, packed_rows, width - LANES), BF16),
        in_specs=[pl.BlockSpec(memory_space=pltpu.VMEM), pl.BlockSpec(memory_space=pl.ANY)],
        compiler_params=params(),
        name="scan_states",
    )(packed, after)


def intra_kernel(q, k, v, pre, out, carried, memory, offset):
    @pl.when(pl.program_id(0) == 0)
    def _():
        memory[...] = jnp.zeros_like(memory)
        offset[...] = jnp.zeros_like(offset)

    width = q.shape[1]
    lower = tri_mask("lower")
    g = log_decay_of(pre[...])
    within = tri_sum(lower.astype(BF16), g)
    final = within[CHUNK - 1 : CHUNK, :]
    middle = within[CHUNK // 2 : CHUNK // 2 + 1, :]
    queries = q[...].astype(F32) * width ** (-0.5)
    keys = k[...].astype(F32)
    values = v[...]
    near_q = (queries * jnp.exp(within - middle)).astype(BF16)
    near_k = (keys * jnp.exp(middle - within)).astype(BF16)
    scores = jnp.where(lower, dot(near_q, near_k, NT), 0.0).astype(BF16)
    decayed_q = queries * jnp.exp(within)
    held = memory[...]
    outside = dot(decayed_q.astype(BF16), held.astype(BF16), NT)
    out[...] = (outside + dot(scores, values)).astype(BF16)
    carried[...] = (decayed_q * jnp.exp(offset[...])).astype(BF16)
    offset[...] = offset[...] + final
    decayed_k = (keys * jnp.exp(final - within)).astype(BF16)
    memory[...] = held * jnp.exp(final) + dot(values, decayed_k, TN)


def intra(q, k, v, pre, name):
    rows, width = q.shape
    value_width = v.shape[1]

    def spec(cols):
        return pl.BlockSpec((CHUNK, cols), lambda i: (i, 0))

    return pl.pallas_call(
        intra_kernel,
        grid=(rows // CHUNK,),
        in_specs=[spec(width), spec(width), spec(value_width), spec(width)],
        out_specs=[spec(value_width), spec(width)],
        out_shape=[
            jax.ShapeDtypeStruct((rows, value_width), BF16),
            jax.ShapeDtypeStruct((rows, width), BF16),
        ],
        scratch_shapes=[pltpu.VMEM((value_width, width), F32), pltpu.VMEM((1, width), F32)],
        compiler_params=params(WIDE, dimension_semantics=("arbitrary",)),
        name=name,
    )(q, k, v, pre)


def gated_of(inside, carried, gate, held, gain):
    att = inside[...].astype(F32) + dot(carried[...], held, NT)
    scale = lax.rsqrt(jnp.mean(jnp.square(att), axis=-1, keepdims=True) + EPS)
    u = gate[...].astype(F32)
    return (att * scale * gain[...] * (u / (1.0 + jnp.exp(-u)))).astype(BF16)


def project_kernel(place, aw, cw, gw, an, cn, gn, state, gain, ow, on, *outs):
    keys_w = cw.shape[1]
    wide = gated_of(aw, cw, gw, state[:, :keys_w], gain)
    narrow = gated_of(an, cn, gn, state[:, keys_w:], gain)
    term = dot(wide, ow[...]) + dot(narrow, on[...])
    half = term.shape[0] // 2
    step = pl.program_id(0)
    if len(outs) == 2:
        outs[0][...] = term[:half].astype(BF16)
        outs[1][...] = term[half:].astype(BF16)
        return

    @pl.when(step == 0)
    def _():
        outs[0][...] = term[:half].astype(BF16)
        outs[1][...] = term[half:].astype(BF16)

    @pl.when(step == 1)
    def _():
        outs[2][...] = term[:half].astype(BF16)
        outs[3][...] = term[half:].astype(BF16)

    @pl.when(step == 2)
    def _():
        outs[4][...] = term


def project(place, arrays, state, gain, ow, on, blocks, turns, name):
    rows = arrays[0].shape[0]
    step = rows // blocks
    full = ow.shape[1]

    def block_of(i, p):
        turn = turns[0]
        for n in range(1, len(turns)):
            turn = jnp.where(i == n, turns[n], turn)
        return lax.rem(p[0] + turn, blocks)

    def spec(a):
        return pl.BlockSpec((step, a.shape[1]), lambda i, p: (block_of(i, p), 0))

    def whole(a):
        return pl.BlockSpec(a.shape, lambda i, p: (0, 0))

    half = jax.ShapeDtypeStruct((step // 2, full), BF16)
    shapes = [half, half]
    if len(turns) > 1:
        shapes = [half] * 4 + [jax.ShapeDtypeStruct((step, full), F32)]
    return pl.pallas_call(
        project_kernel,
        grid_spec=pltpu.PrefetchScalarGridSpec(
            num_scalar_prefetch=1,
            grid=(len(turns),),
            in_specs=[spec(a) for a in arrays] + [whole(a) for a in (state, gain, ow, on)],
            out_specs=[whole(o) for o in shapes],
        ),
        out_shape=shapes,
        compiler_params=params(dimension_semantics=("arbitrary",)),
        name=name,
    )(place, *arrays, state, gain, ow, on)


def add_kernel(a, b, c, d, first, second):
    first[...] = (a[...].astype(F32) + b[...].astype(F32)).astype(BF16)
    second[...] = (c[...].astype(F32) + d[...].astype(F32)).astype(BF16)


def add_pairs(a, b, c, d):
    shape = jax.ShapeDtypeStruct(a.shape, BF16)
    return pl.pallas_call(
        add_kernel, out_shape=[shape, shape], compiler_params=params(), name="add_pairs"
    )(a, b, c, d)


def stream_kernel(place, own, prev_low, prev_high, next_low, next_high, residual, gain, stream, normed):
    half = prev_low.shape[0]
    for at, first, second in ((0, prev_low, next_low), (half, prev_high, next_high)):
        span = slice(at, at + half)
        mixed = own[span, :] + first[...].astype(F32) + second[...].astype(F32)
        held = (residual[span, :].astype(F32) + mixed).astype(BF16)
        stream[span, :] = held
        wide = held.astype(F32)
        scale = lax.rsqrt(jnp.mean(jnp.square(wide), axis=-1, keepdims=True) + EPS)
        normed[span, :] = (wide * scale * gain[...]).astype(BF16)


def make_stream(place, own, pieces, residual, gain):
    rows, full = own.shape

    def whole(a):
        return pl.BlockSpec(a.shape, lambda i, p: (0, 0))

    return pl.pallas_call(
        stream_kernel,
        grid_spec=pltpu.PrefetchScalarGridSpec(
            num_scalar_prefetch=1,
            grid=(1,),
            in_specs=[
                whole(own),
                *[whole(a) for a in pieces],
                pl.BlockSpec((rows, full), lambda i, p: (p[0], 0)),
                whole(gain),
            ],
            out_specs=[pl.BlockSpec((rows, full), lambda i, p: (0, 0))] * 2,
        ),
        out_shape=[jax.ShapeDtypeStruct((rows, full), BF16)] * 2,
        compiler_params=params(dimension_semantics=("arbitrary",)),
        name="make_stream",
    )(place, own, *pieces, residual, gain)


def mixer_kernel(place, normed, stream, weights, *refs):
    *outs, held_up, held_down, hidden, up_sems, down_sems = refs
    count, n_sp, each, width = held_up.shape
    blocks, per_block, n_x, _, cols = held_down.shape
    per = cols // width
    full = normed.shape[1]
    block_cols = per_block * each
    ups, downs = [], []
    for s in range(count):
        source = weights.at[:, s // per, 0:each, pl.ds((s % per) * width, width)]
        ups.append(pltpu.make_async_copy(source, held_up.at[s], up_sems.at[s]))
    turns = (2, 1, 3, 0)
    for b, turn in enumerate(turns):
        block = lax.rem(place[0] + turn, blocks)
        source = weights.at[pl.ds(block * per_block, per_block), :, each : 2 * each, :]
        downs.append(pltpu.make_async_copy(source, held_down.at[b], down_sems.at[b]))
    for copy in ups + downs:
        copy.start()
    for s in range(count):
        ups[s].wait()
        before = dot(normed[...], held_up[s].reshape(full, width))
        hidden[:, s * width : (s + 1) * width] = jnp.square(jnp.maximum(before, 0.0)).astype(BF16)
    for b, turn in enumerate(turns):
        downs[b].wait()
        block = lax.rem(place[0] + turn, blocks)
        start = pl.multiple_of(block * block_cols, block_cols)
        total = stream[:, pl.ds(start, block_cols)].astype(F32)
        for x in range(n_x):
            total = total + dot(
                hidden[:, x * cols : (x + 1) * cols],
                held_down[b, :, x].reshape(block_cols, cols),
                NT,
            )
        outs[b][...] = total.astype(BF16)


def mixer(place, normed, stream, weights, count, width):
    rows, full = normed.shape
    n_sp, n_x, both, cols = weights.shape
    each = both // 2
    steps = n_x * cols // width
    vmem = pl.BlockSpec(memory_space=pltpu.VMEM)
    return pl.pallas_call(
        mixer_kernel,
        in_specs=[
            pl.BlockSpec(memory_space=pltpu.SMEM),
            vmem,
            vmem,
            pl.BlockSpec(memory_space=pl.ANY),
        ],
        out_shape=[jax.ShapeDtypeStruct((rows, full // count), BF16)] * count,
        scratch_shapes=[
            pltpu.VMEM((steps, n_sp, each, width), BF16),
            pltpu.VMEM((count, n_sp // count, n_x, each, cols), BF16),
            pltpu.VMEM((rows, n_x * cols), BF16),
            pltpu.SemaphoreType.DMA((steps,)),
            pltpu.SemaphoreType.DMA((count,)),
        ],
        compiler_params=params(44),
        name="mixer",
    )(place, normed, stream, weights)


def stacked_kernel(first, second, out):
    rows = first.shape[0]
    out[0:rows, :] = first[...]
    out[rows:, :] = second[...]


def stacked_rows(first, second):
    rows, cols = first.shape
    return pl.pallas_call(
        stacked_kernel,
        out_shape=jax.ShapeDtypeStruct((2 * rows, cols), BF16),
        compiler_params=params(WIDE),
        name="stacked_rows",
    )(first, second)


def rows_kernel(place, *refs):
    *pieces, out = refs
    rows = pieces[0].shape[0]
    for r, piece in enumerate(pieces):
        block = lax.rem(place[0] - r + len(pieces), len(pieces))
        out[pl.ds(pl.multiple_of(block * rows, rows), rows), :] = piece[...]


def gather_rows(place, pieces):
    rows, cols = pieces[0].shape
    return pl.pallas_call(
        rows_kernel,
        in_specs=[pl.BlockSpec(memory_space=pltpu.SMEM)]
        + [pl.BlockSpec(memory_space=pltpu.VMEM)] * len(pieces),
        out_shape=jax.ShapeDtypeStruct((len(pieces) * rows, cols), BF16),
        compiler_params=params(8),
        name="gather_rows",
    )(place, *pieces)


def shifted(array, axis, step):
    count = lax.axis_size(axis)
    return lax.ppermute(array, axis, [(i, (i + step) % count) for i in range(count)])


def near(array):
    return pltpu.with_memory_space_constraint(array, pltpu.VMEM)


def away(array):
    return pltpu.with_memory_space_constraint(array, pltpu.HBM)


def held_until(arrays, *others):
    return list(lax.optimization_barrier((tuple(arrays), others))[0])


def body(
    residual,
    query_wide,
    key_wide,
    value_wide,
    decay_wide,
    gate_wide,
    query_narrow,
    key_narrow,
    value_narrow,
    decay_narrow,
    gate_narrow,
    head_gain,
    out_wide,
    out_narrow,
    mlp_gain,
    up_weight,
    down_weight,
):
    n_x = lax.axis_size("x")
    line = ("z", "y", "c")
    n_sp = lax.axis_size(line)
    rows, full = residual.shape
    place = lax.axis_index("x").astype(jnp.int32).reshape(1)
    own = stacked_rows(up_weight, down_weight.T)
    weights = lax.all_gather(own, (*line, "x"), axis=0, tiled=False)
    weights = weights.reshape(n_sp, n_x, *own.shape)
    packed = local_state(
        key_wide, decay_wide, value_wide, key_narrow, decay_narrow, value_narrow, n_sp
    )
    received = lax.all_to_all(packed, line, 0, 0, tiled=True)
    wide_in, wide_q = intra(query_wide, key_wide, value_wide, decay_wide, "intra_wide")
    entering = scan_states(near(received), away(wide_q))
    arrived = lax.all_to_all(entering, line, 0, 0, tiled=True)
    (query_narrow,) = held_until([query_narrow], entering)
    narrow_in, narrow_q = intra(
        query_narrow, key_narrow, value_narrow, decay_narrow, "intra_narrow"
    )
    (arrived,) = held_until([arrived], narrow_q)
    state = near(arrived.reshape(-1, arrived.shape[2]))
    arrays = tuple(
        away(a) for a in (wide_in, wide_q, gate_wide, narrow_in, narrow_q, gate_narrow)
    )
    rest = (state, head_gain.reshape(1, -1), away(out_wide), away(out_narrow), n_x)
    far_low, far_high = project(place, arrays, *rest, (2,), "project_far")
    from_prev = shifted(far_low, "x", 1)
    from_next = shifted(far_high, "x", -1)
    next_low, next_high, prev_low, prev_high, own = project(
        place, arrays, *rest, (1, 3, 0), "project_near"
    )
    high_of_prev = shifted(next_high, "x", 1)
    low_of_next = shifted(prev_low, "x", -1)
    next_low, prev_high = add_pairs(next_low, near(from_prev), prev_high, near(from_next))
    low_of_prev = shifted(next_low, "x", 1)
    high_of_next = shifted(prev_high, "x", -1)
    stream, normed = make_stream(
        place,
        own,
        tuple(near(a) for a in (low_of_prev, high_of_prev, low_of_next, high_of_next)),
        away(residual),
        mlp_gain.reshape(1, -1),
    )
    opposite, after, before, kept = mixer(place, near(normed), near(stream), weights, n_x, 512)
    opposite = shifted(opposite, "x", 2)
    after = shifted(after, "x", 1)
    before = shifted(before, "x", -1)
    return gather_rows(place, (near(kept), near(after), near(opposite), near(before)))


def solution(mesh):
    n_tp = mesh.shape["tp"]
    side = int(round((mesh.shape["sp"] // 2) ** 0.5))
    cut = Mesh(mesh.devices.reshape(side, side, 2, n_tp), ("z", "y", "c", "x"))
    line = ("z", "y", "c")
    step = jax.shard_map(
        body,
        mesh=cut,
        in_specs=(
            P(line, None),
            P(line, "x"),
            P(line, "x"),
            P(line, "x"),
            P(line, "x"),
            P(line, "x"),
            P(line, "x"),
            P(line, "x"),
            P(line, "x"),
            P(line, "x"),
            P(line, "x"),
            P(),
            P("x", None),
            P("x", None),
            P(),
            P(line, "x"),
            P("x", line),
        ),
        out_specs=P(line, "x"),
        check_vma=False,
    )
    return step
```

```python
import jax
import jax.numpy as jnp
from jax import lax
from jax.experimental import pallas as pl
from jax.experimental.pallas import tpu as pltpu
from jax.sharding import Mesh, PartitionSpec as P

EPS = 1e-05
DECAY_NORMALIZER = 16.0
CHUNK = 128
F32 = jnp.float32
BF16 = jnp.bfloat16
NT = (((1,), (1,)), ((), ()))
TN = (((0,), (0,)), ((), ()))
LANES = 128
IN_FLIGHT = 4
WIDE = 58


def dot(a, b, dims=(((1,), (0,)), ((), ()))):
    return lax.dot_general(a, b, dims, preferred_element_type=F32)


def log_decay_of(pre):
    x = pre.astype(F32)
    return (jnp.minimum(x, 0.0) - jnp.log1p(jnp.exp(-jnp.abs(x)))) / DECAY_NORMALIZER


def tri_sum(tri, g):
    high = g.astype(BF16)
    low = (g - high.astype(F32)).astype(BF16)
    return dot(tri, high) + dot(tri, low)


def tri_mask(kind):
    row = lax.broadcasted_iota(jnp.int32, (CHUNK, CHUNK), 0)
    col = lax.broadcasted_iota(jnp.int32, (CHUNK, CHUNK), 1)
    return (col <= row) if kind == "lower" else (col > row)


def params(mib=24, **kw):
    return pltpu.CompilerParams(vmem_limit_bytes=mib * 1024 * 1024, **kw)


def state_kernel(kw, dw, vw, kn, dn, vn, packed, decayed_w, decayed_n):
    later = tri_mask("upper").astype(BF16)
    rows = kw.shape[0]
    keys_w = kw.shape[1]
    for key, pre, decayed, value, at in (
        (kw, dw, decayed_w, vw, 0),
        (kn, dn, decayed_n, vn, keys_w),
    ):
        width = key.shape[1]
        offset = jnp.zeros((1, width), F32)
        for block in reversed(range(rows // CHUNK)):
            span = pl.ds(block * CHUNK, CHUNK)
            g = log_decay_of(pre[span, :])
            after = tri_sum(later, g)
            decayed[span, :] = (key[span, :].astype(F32) * jnp.exp(after + offset)).astype(BF16)
            offset = offset + after[0:1, :] + g[0:1, :]
        state = dot(value[...], decayed[...], TN)
        slices = packed.shape[0]
        state_rows = state.shape[0] // slices
        packed[:, :, at : at + width] = state.astype(BF16).reshape(slices, state_rows, width)
        decay = jnp.exp(offset).astype(BF16)
        for lane in range(0, width, LANES):
            row = (at + lane) // LANES
            packed[:, row : row + 1, -LANES:] = jnp.broadcast_to(
                decay[None, :, lane : lane + LANES], (slices, 1, LANES)
            )


def local_state(kw, dw, vw, kn, dn, vn, slices):
    rows, keys_w = kw.shape
    keys_n = kn.shape[1]
    state_rows = vw.shape[1] // slices
    return pl.pallas_call(
        state_kernel,
        out_shape=jax.ShapeDtypeStruct((slices, state_rows, keys_w + keys_n + LANES), BF16),
        scratch_shapes=[pltpu.VMEM((rows, keys_w), BF16), pltpu.VMEM((rows, keys_n), BF16)],
        compiler_params=params(WIDE),
        name="local_state",
    )(kw, dw, vw, kn, dn, vn)


def scan_kernel(packed, after, entering):
    slices, state_rows, width = entering.shape
    state = jnp.zeros((state_rows, width), F32)
    for i in range(slices):
        entering[i] = state.astype(BF16)
        if i + 1 < slices:
            decay = jnp.concatenate(
                [packed[i, r : r + 1, width:].astype(F32) for r in range(width // LANES)], axis=1
            )
            state = state * decay + packed[i, :, 0:width].astype(F32)


def scan_states(packed, after):
    slices, packed_rows, width = packed.shape
    return pl.pallas_call(
        scan_kernel,
        out_shape=jax.ShapeDtypeStruct((slices, packed_rows, width - LANES), BF16),
        in_specs=[pl.BlockSpec(memory_space=pltpu.VMEM), pl.BlockSpec(memory_space=pl.ANY)],
        compiler_params=params(),
        name="scan_states",
    )(packed, after)


def intra_kernel(q, k, v, pre, out, carried, memory, offset):
    @pl.when(pl.program_id(0) == 0)
    def _():
        memory[...] = jnp.zeros_like(memory)
        offset[...] = jnp.zeros_like(offset)

    width = q.shape[1]
    lower = tri_mask("lower")
    g = log_decay_of(pre[...])
    within = tri_sum(lower.astype(BF16), g)
    final = within[CHUNK - 1 : CHUNK, :]
    middle = within[CHUNK // 2 : CHUNK // 2 + 1, :]
    queries = q[...].astype(F32) * width ** (-0.5)
    keys = k[...].astype(F32)
    values = v[...]
    near_q = (queries * jnp.exp(within - middle)).astype(BF16)
    near_k = (keys * jnp.exp(middle - within)).astype(BF16)
    scores = jnp.where(lower, dot(near_q, near_k, NT), 0.0).astype(BF16)
    decayed_q = queries * jnp.exp(within)
    held = memory[...]
    outside = dot(decayed_q.astype(BF16), held.astype(BF16), NT)
    out[...] = (outside + dot(scores, values)).astype(BF16)
    carried[...] = (decayed_q * jnp.exp(offset[...])).astype(BF16)
    offset[...] = offset[...] + final
    decayed_k = (keys * jnp.exp(final - within)).astype(BF16)
    memory[...] = held * jnp.exp(final) + dot(values, decayed_k, TN)


def intra(q, k, v, pre, name):
    rows, width = q.shape
    value_width = v.shape[1]

    def spec(cols):
        return pl.BlockSpec((CHUNK, cols), lambda i: (i, 0))

    return pl.pallas_call(
        intra_kernel,
        grid=(rows // CHUNK,),
        in_specs=[spec(width), spec(width), spec(value_width), spec(width)],
        out_specs=[spec(value_width), spec(width)],
        out_shape=[
            jax.ShapeDtypeStruct((rows, value_width), BF16),
            jax.ShapeDtypeStruct((rows, width), BF16),
        ],
        scratch_shapes=[pltpu.VMEM((value_width, width), F32), pltpu.VMEM((1, width), F32)],
        compiler_params=params(WIDE, dimension_semantics=("arbitrary",)),
        name=name,
    )(q, k, v, pre)


def gated_of(inside, carried, gate, held, gain):
    att = inside[...].astype(F32) + dot(carried[...], held, NT)
    scale = lax.rsqrt(jnp.mean(jnp.square(att), axis=-1, keepdims=True) + EPS)
    u = gate[...].astype(F32)
    return (att * scale * gain[...] * (u / (1.0 + jnp.exp(-u)))).astype(BF16)


def project_kernel(place, aw, cw, gw, an, cn, gn, state, gain, ow, on, *outs):
    keys_w = cw.shape[1]
    wide = gated_of(aw, cw, gw, state[:, :keys_w], gain)
    narrow = gated_of(an, cn, gn, state[:, keys_w:], gain)
    term = dot(wide, ow[...]) + dot(narrow, on[...])
    half = term.shape[0] // 2
    step = pl.program_id(0)
    if len(outs) == 2:
        outs[0][...] = term[:half].astype(BF16)
        outs[1][...] = term[half:].astype(BF16)
        return

    @pl.when(step == 0)
    def _():
        outs[0][...] = term[:half].astype(BF16)
        outs[1][...] = term[half:].astype(BF16)

    @pl.when(step == 1)
    def _():
        outs[2][...] = term[:half].astype(BF16)
        outs[3][...] = term[half:].astype(BF16)

    @pl.when(step == 2)
    def _():
        outs[4][...] = term


def project(place, arrays, state, gain, ow, on, blocks, turns, name):
    rows = arrays[0].shape[0]
    step = rows // blocks
    full = ow.shape[1]

    def block_of(i, p):
        turn = turns[0]
        for n in range(1, len(turns)):
            turn = jnp.where(i == n, turns[n], turn)
        return lax.rem(p[0] + turn, blocks)

    def spec(a):
        return pl.BlockSpec((step, a.shape[1]), lambda i, p: (block_of(i, p), 0))

    def whole(a):
        return pl.BlockSpec(a.shape, lambda i, p: (0, 0))

    half = jax.ShapeDtypeStruct((step // 2, full), BF16)
    shapes = [half, half]
    if len(turns) > 1:
        shapes = [half] * 4 + [jax.ShapeDtypeStruct((step, full), F32)]
    return pl.pallas_call(
        project_kernel,
        grid_spec=pltpu.PrefetchScalarGridSpec(
            num_scalar_prefetch=1,
            grid=(len(turns),),
            in_specs=[spec(a) for a in arrays] + [whole(a) for a in (state, gain, ow, on)],
            out_specs=[whole(o) for o in shapes],
        ),
        out_shape=shapes,
        compiler_params=params(dimension_semantics=("arbitrary",)),
        name=name,
    )(place, *arrays, state, gain, ow, on)


def add_kernel(a, b, c, d, first, second):
    first[...] = (a[...].astype(F32) + b[...].astype(F32)).astype(BF16)
    second[...] = (c[...].astype(F32) + d[...].astype(F32)).astype(BF16)


def add_pairs(a, b, c, d):
    shape = jax.ShapeDtypeStruct(a.shape, BF16)
    return pl.pallas_call(
        add_kernel, out_shape=[shape, shape], compiler_params=params(), name="add_pairs"
    )(a, b, c, d)


def stream_kernel(place, own, prev_low, prev_high, next_low, next_high, residual, gain, stream, normed):
    half = prev_low.shape[0]
    for at, first, second in ((0, prev_low, next_low), (half, prev_high, next_high)):
        span = slice(at, at + half)
        mixed = own[span, :] + first[...].astype(F32) + second[...].astype(F32)
        held = (residual[span, :].astype(F32) + mixed).astype(BF16)
        stream[span, :] = held
        wide = held.astype(F32)
        scale = lax.rsqrt(jnp.mean(jnp.square(wide), axis=-1, keepdims=True) + EPS)
        normed[span, :] = (wide * scale * gain[...]).astype(BF16)


def make_stream(place, own, pieces, residual, gain):
    rows, full = own.shape

    def whole(a):
        return pl.BlockSpec(a.shape, lambda i, p: (0, 0))

    return pl.pallas_call(
        stream_kernel,
        grid_spec=pltpu.PrefetchScalarGridSpec(
            num_scalar_prefetch=1,
            grid=(1,),
            in_specs=[
                whole(own),
                *[whole(a) for a in pieces],
                pl.BlockSpec((rows, full), lambda i, p: (p[0], 0)),
                whole(gain),
            ],
            out_specs=[pl.BlockSpec((rows, full), lambda i, p: (0, 0))] * 2,
        ),
        out_shape=[jax.ShapeDtypeStruct((rows, full), BF16)] * 2,
        compiler_params=params(dimension_semantics=("arbitrary",)),
        name="make_stream",
    )(place, own, *pieces, residual, gain)


def mixer_kernel(place, normed, stream, weights, *refs):
    *outs, held_up, held_down, hidden, up_sems, down_sems = refs
    count, n_sp, each, width = held_up.shape
    blocks, per_block, n_x, _, cols = held_down.shape
    per = cols // width
    full = normed.shape[1]
    block_cols = per_block * each
    ups, downs = [], []
    for s in range(count):
        source = weights.at[:, s // per, 0:each, pl.ds((s % per) * width, width)]
        ups.append(pltpu.make_async_copy(source, held_up.at[s], up_sems.at[s]))
    turns = (2, 1, 3, 0)
    for b, turn in enumerate(turns):
        block = lax.rem(place[0] + turn, blocks)
        source = weights.at[pl.ds(block * per_block, per_block), :, each : 2 * each, :]
        downs.append(pltpu.make_async_copy(source, held_down.at[b], down_sems.at[b]))
    queue = ups + downs
    for copy in queue[:IN_FLIGHT]:
        copy.start()

    def arrive(i):
        queue[i].wait()
        if i + IN_FLIGHT < len(queue):
            queue[i + IN_FLIGHT].start()

    for s in range(count):
        arrive(s)
        before = dot(normed[...], held_up[s].reshape(full, width))
        hidden[:, s * width : (s + 1) * width] = jnp.square(jnp.maximum(before, 0.0)).astype(BF16)
    for b, turn in enumerate(turns):
        arrive(count + b)
        block = lax.rem(place[0] + turn, blocks)
        start = pl.multiple_of(block * block_cols, block_cols)
        total = stream[:, pl.ds(start, block_cols)].astype(F32)
        for x in range(n_x):
            total = total + dot(
                hidden[:, x * cols : (x + 1) * cols],
                held_down[b, :, x].reshape(block_cols, cols),
                NT,
            )
        outs[b][...] = total.astype(BF16)


def mixer(place, normed, stream, weights, count, width):
    rows, full = normed.shape
    n_sp, n_x, both, cols = weights.shape
    each = both // 2
    steps = n_x * cols // width
    vmem = pl.BlockSpec(memory_space=pltpu.VMEM)
    return pl.pallas_call(
        mixer_kernel,
        in_specs=[
            pl.BlockSpec(memory_space=pltpu.SMEM),
            vmem,
            vmem,
            pl.BlockSpec(memory_space=pl.ANY),
        ],
        out_shape=[jax.ShapeDtypeStruct((rows, full // count), BF16)] * count,
        scratch_shapes=[
            pltpu.VMEM((steps, n_sp, each, width), BF16),
            pltpu.VMEM((count, n_sp // count, n_x, each, cols), BF16),
            pltpu.VMEM((rows, n_x * cols), BF16),
            pltpu.SemaphoreType.DMA((steps,)),
            pltpu.SemaphoreType.DMA((count,)),
        ],
        compiler_params=params(44),
        name="mixer",
    )(place, normed, stream, weights)


def stacked_kernel(first, second, out):
    rows = first.shape[0]
    out[0:rows, :] = first[...]
    out[rows:, :] = second[...]


def stacked_rows(first, second):
    rows, cols = first.shape
    return pl.pallas_call(
        stacked_kernel,
        out_shape=jax.ShapeDtypeStruct((2 * rows, cols), BF16),
        compiler_params=params(WIDE),
        name="stacked_rows",
    )(first, second)


def rows_kernel(place, *refs):
    *pieces, out = refs
    rows = pieces[0].shape[0]
    for r, piece in enumerate(pieces):
        block = lax.rem(place[0] - r + len(pieces), len(pieces))
        out[pl.ds(pl.multiple_of(block * rows, rows), rows), :] = piece[...]


def gather_rows(place, pieces):
    rows, cols = pieces[0].shape
    return pl.pallas_call(
        rows_kernel,
        in_specs=[pl.BlockSpec(memory_space=pltpu.SMEM)]
        + [pl.BlockSpec(memory_space=pltpu.VMEM)] * len(pieces),
        out_shape=jax.ShapeDtypeStruct((len(pieces) * rows, cols), BF16),
        compiler_params=params(8),
        name="gather_rows",
    )(place, *pieces)


def shifted(array, axis, step):
    count = lax.axis_size(axis)
    return lax.ppermute(array, axis, [(i, (i + step) % count) for i in range(count)])


def near(array):
    return pltpu.with_memory_space_constraint(array, pltpu.VMEM)


def away(array):
    return pltpu.with_memory_space_constraint(array, pltpu.HBM)


def held_until(arrays, *others):
    return list(lax.optimization_barrier((tuple(arrays), others))[0])


def body(
    residual,
    query_wide,
    key_wide,
    value_wide,
    decay_wide,
    gate_wide,
    query_narrow,
    key_narrow,
    value_narrow,
    decay_narrow,
    gate_narrow,
    head_gain,
    out_wide,
    out_narrow,
    mlp_gain,
    up_weight,
    down_weight,
):
    n_x = lax.axis_size("x")
    line = ("z", "y", "c")
    n_sp = lax.axis_size(line)
    rows, full = residual.shape
    place = lax.axis_index("x").astype(jnp.int32).reshape(1)
    own = stacked_rows(up_weight, down_weight.T)
    weights = lax.all_gather(own, (*line, "x"), axis=0, tiled=False)
    weights = weights.reshape(n_sp, n_x, *own.shape)
    packed = local_state(
        key_wide, decay_wide, value_wide, key_narrow, decay_narrow, value_narrow, n_sp
    )
    received = lax.all_to_all(packed, line, 0, 0, tiled=True)
    wide_in, wide_q = intra(query_wide, key_wide, value_wide, decay_wide, "intra_wide")
    entering = scan_states(near(received), away(wide_q))
    arrived = lax.all_to_all(entering, line, 0, 0, tiled=True)
    (query_narrow,) = held_until([query_narrow], entering)
    narrow_in, narrow_q = intra(
        query_narrow, key_narrow, value_narrow, decay_narrow, "intra_narrow"
    )
    (arrived,) = held_until([arrived], narrow_q)
    state = near(arrived.reshape(-1, arrived.shape[2]))
    arrays = tuple(
        away(a) for a in (wide_in, wide_q, gate_wide, narrow_in, narrow_q, gate_narrow)
    )
    rest = (state, head_gain.reshape(1, -1), away(out_wide), away(out_narrow), n_x)
    far_low, far_high = project(place, arrays, *rest, (2,), "project_far")
    from_prev = shifted(far_low, "x", 1)
    from_next = shifted(far_high, "x", -1)
    next_low, next_high, prev_low, prev_high, own = project(
        place, arrays, *rest, (1, 3, 0), "project_near"
    )
    high_of_prev = shifted(next_high, "x", 1)
    low_of_next = shifted(prev_low, "x", -1)
    next_low, prev_high = add_pairs(next_low, near(from_prev), prev_high, near(from_next))
    low_of_prev = shifted(next_low, "x", 1)
    high_of_next = shifted(prev_high, "x", -1)
    stream, normed = make_stream(
        place,
        own,
        tuple(near(a) for a in (low_of_prev, high_of_prev, low_of_next, high_of_next)),
        away(residual),
        mlp_gain.reshape(1, -1),
    )
    opposite, after, before, kept = mixer(place, near(normed), near(stream), weights, n_x, 512)
    opposite = shifted(opposite, "x", 2)
    after = shifted(after, "x", 1)
    before = shifted(before, "x", -1)
    return gather_rows(place, (near(kept), near(after), near(opposite), near(before)))


def solution(mesh):
    n_tp = mesh.shape["tp"]
    side = int(round((mesh.shape["sp"] // 2) ** 0.5))
    cut = Mesh(mesh.devices.reshape(side, side, 2, n_tp), ("z", "y", "c", "x"))
    line = ("z", "y", "c")
    step = jax.shard_map(
        body,
        mesh=cut,
        in_specs=(
            P(line, None),
            P(line, "x"),
            P(line, "x"),
            P(line, "x"),
            P(line, "x"),
            P(line, "x"),
            P(line, "x"),
            P(line, "x"),
            P(line, "x"),
            P(line, "x"),
            P(line, "x"),
            P(),
            P("x", None),
            P("x", None),
            P(),
            P(line, "x"),
            P("x", line),
        ),
        out_specs=P(line, "x"),
        check_vma=False,
    )
    return step
```
